512 devices in a mesh: ep: 32 (over z, core), tp: 16 (over y, x).
Axes of the slice: x: 4, y: 4, z: 16, core: 2. Of those that a mesh axis runs over, the one named last changes fastest.
Arguments:
- mixer_rows: bfloat16 [8192, 2048], P('ep'), may hold values from -8 to 8
- mixer_gain: float32 [2048], replicated, may hold values from 0.1 to 1.9
- w_query: bfloat16 [2048, 1024], P(None, 'tp'), may hold values from -0.125 to 0.125
- w_key: bfloat16 [2048, 1024], P(None, 'tp'), may hold values from -0.125 to 0.125
- w_value: bfloat16 [2048, 1024], P(None, 'tp'), may hold values from -0.125 to 0.125
- key_shift: float32 [16, 8192], P('tp'), may hold values from -14 to 0
- w_out: bfloat16 [1024, 2048], P(None, 'tp'), may hold values from -0.75 to 0.75
- expert_rows: bfloat16 [4096, 2048], P('ep'), may hold values from -6 to 6
- expert_gain: float32 [2048], replicated, may hold values from 0.1 to 1.9
- routes: int32 [4096, 4], P('ep'), may hold values from 0 to 31, all different within a row; in each aligned block of 128 rows (0 to 127, 128 to 255, ...) at most 32 rows name the same one
- route_weight: float32 [4096, 4], P('ep'), may hold values from 0.05 to 0.6
- w_gate: bfloat16 [32, 2048, 2048], P('ep', None, 'tp'), may hold values from -0.25 to 0.25
- w_up: bfloat16 [32, 2048, 2048], P('ep', None, 'tp'), may hold values from -0.25 to 0.25
- w_down: bfloat16 [32, 2048, 2048], P('ep', None, 'tp'), may hold values from -0.0625 to 0.0625
Outputs:
- mixer_out: bfloat16 [8192, 2048], P('ep', 'tp')
- expert_out: bfloat16 [4096, 2048], P('ep', 'tp')
The draws below stay inside these ranges and needn't reach their ends.
Inputs may be any that keep to these rules, and one draw needn't show every extreme that they name: `routes`: each row names 4 different experts. In each aligned block of 128 rows no expert is named by more than 32 rows, and in every draw some block names some expert exactly 32 times.
All inputs are finite; a program needn't handle non-finite values.
Results may differ from the reference program's by a relative error of at most 0.0073.
Values may be sent and summed in bfloat16 or wider, within the bound.
A program may use at most 64 MiB of HBM per device.

```python
import math
import jax
import jax.numpy as jnp
import numpy as np
from jax import lax

D = 2048
HEAD_TOTAL = 16
HEAD_DIM = 64
FF = 2048
TOPK = 4
TOKA_DEV = 256
TOKB_DEV = 128
SEQUENCE_TOKENS = 8192
TOKB = 4096
EXPERTS = 32
CAP = 32
N_EP = 32


def draw_mixer_rows(key, part):
    parallel_lanes = jax.random.split(key, 2)
    block_count = SEQUENCE_TOKENS // TOKA_DEV
    baseline = jax.random.normal(parallel_lanes[0], (SEQUENCE_TOKENS, D), jnp.float32)
    common = jax.random.normal(parallel_lanes[1], (block_count, D), jnp.float32)
    values = baseline + jnp.repeat(common, TOKA_DEV, axis=0)
    return jnp.clip(values, -8.0, 8.0).astype(jnp.bfloat16)


def draw_key_shift(key, part):
    parallel_lanes = jax.random.split(key, 7)
    block_count = SEQUENCE_TOKENS // TOKA_DEV
    fast_share = 0.5
    head_pick = jax.random.uniform(parallel_lanes[0], (HEAD_TOTAL, 1), jnp.float32)
    fast_span = jnp.exp(jax.random.uniform(parallel_lanes[1], (HEAD_TOTAL, 1), jnp.float32, 3.4, 4.6))
    slow_span = SEQUENCE_TOKENS * jax.random.uniform(parallel_lanes[2], (HEAD_TOTAL, 1), jnp.float32, 1.0, 2.0)
    baseline = -jnp.log(jnp.where(head_pick < fast_share, fast_span, slow_span))
    block_level = jax.random.uniform(parallel_lanes[3], (HEAD_TOTAL, block_count), jnp.float32, -0.7, 0.7)
    roughness = jax.random.uniform(parallel_lanes[4], (HEAD_TOTAL, SEQUENCE_TOKENS), jnp.float32, -0.5, 0.5)
    displaced_values = baseline + jnp.repeat(block_level, TOKA_DEV, axis=1) + roughness
    surge_selection = jax.random.uniform(parallel_lanes[5], (1, SEQUENCE_TOKENS), jnp.float32) < 4.0 / SEQUENCE_TOKENS
    surge_degree = jax.random.uniform(parallel_lanes[6], (HEAD_TOTAL, SEQUENCE_TOKENS), jnp.float32, -1.4, 0.0)
    return jnp.where(surge_selection, surge_degree, displaced_values).astype(jnp.float32)


def steps_of(own_key, extent, cuts, least, largest):
    loudness = 1.0
    for position, shards_of in cuts:
        draws = jax.random.uniform(jax.random.fold_in(jax.random.fold_in(own_key, 6), position), (shards_of,), jnp.float32, least / len(cuts), largest / len(cuts))
        loudness = loudness * jnp.repeat(jnp.exp(draws), extent[position] // shards_of).reshape((-1,) + (1,) * (len(extent) - 1 - position))
    return loudness


def shared_out(key, own, number, rows, number_of, top, reach, slope):
    sequence = jax.random.permutation(key, number_of)
    crowded, usual = shares(number_of, rows * top, reach, slope, True), shares(number_of, rows * top, reach, slope, False)
    places = jnp.arange(number_of)

    def named(lengths, turn):
        used = int((lengths > 0).sum())
        fixed = max(1, used // 4)
        passed = fixed + (places - fixed + turn * (used - fixed)) % max(1, number_of - fixed)
        return jnp.zeros((number_of,), jnp.int32).at[sequence[jnp.where(places < fixed, places, passed)]].set(jnp.asarray(lengths, jnp.int32))

    lengths = jnp.where(number % 4 == 0, named(crowded, number // 4), named(usual, number - number // 4 - 1))
    mixed = jax.random.permutation(jax.random.fold_in(own, 3), number_of)
    source_of, sink = mixed[0:number_of // 2 * 2:2], mixed[1:number_of // 2 * 2:2]
    slack = jnp.minimum(lengths[source_of] - 1, reach - lengths[sink]) // 2
    slack = jnp.where((source_of == sequence[0]) | (sink == sequence[0]) | (lengths[sink] == 0), 0, jnp.maximum(slack, 0))
    passed = jax.random.randint(jax.random.fold_in(own, 4), (number_of // 2,), 0, 1 << 20) % (slack + 1)
    lengths = lengths.at[source_of].add(-passed).at[sink].add(passed)
    labels = jnp.searchsorted(jnp.cumsum(lengths), jnp.arange(rows * top), side="right").astype(jnp.int32)
    grid = labels.reshape(top, rows).T
    grid = grid[jax.random.permutation(jax.random.fold_in(own, 1), rows)]
    turn = jax.random.randint(jax.random.fold_in(own, 2), (rows, 1), 0, top)
    return jnp.take_along_axis(grid, (jnp.arange(top)[None, :] + turn) % top, axis=1)


def shares(amount, total, reach, slope, full):
    portions = [(1 << 20) // math.isqrt(rank ** slope) + 1 for rank in range(1, amount + 1)]
    largest = reach if full else min(reach, max(-(-total // amount), total * portions[0] // sum(portions)))
    least = 1 if total - largest >= amount - 1 else 0
    holding, spare = [largest] + [least] * (amount - 1), total - largest - least * (amount - 1)
    while spare > 0:
        movable = [i for i in range(1, amount) if holding[i] < largest] or [i for i in range(1, amount) if holding[i] < reach]
        mass, left = sum([portions[i] for i in movable]), spare
        for i in movable:
            more = min(reach - holding[i], max(1, left * portions[i] // mass), spare)
            holding[i] = holding[i] + more
            spare = spare - more
    return np.array(holding)


def gaussian(key, extent, deviation, reach, cuts=(), held_as=jnp.bfloat16):
    array = deviation * jax.random.normal(key, extent, jnp.float32)
    if cuts:
        array = array * steps_of(key, extent, cuts, -0.22, 0.18)
    return jnp.clip(array, -reach, reach).astype(held_as)


def setup_inputs(seed: int = 0) -> dict:
    streams_of = jax.random.split(jax.random.key(seed), 15)
    mixer_rows = draw_mixer_rows(jax.random.fold_in(streams_of[14], 71), 0)
    mixer_gain = jnp.clip(1.0 + 0.18 * jax.random.normal(streams_of[1], (D,), jnp.float32), 0.1, 1.9)
    w_query = gaussian(streams_of[2], (D, HEAD_TOTAL * HEAD_DIM), D ** -0.5, 0.125, ((1, 16),))
    w_key = gaussian(streams_of[3], (D, HEAD_TOTAL * HEAD_DIM), D ** -0.5, 0.125, ((1, 16),))
    w_value = gaussian(streams_of[4], (D, HEAD_TOTAL * HEAD_DIM), D ** -0.5, 0.125, ((1, 16),))
    key_shift = draw_key_shift(jax.random.fold_in(streams_of[14], 71), 0)
    w_out = gaussian(streams_of[6], (HEAD_TOTAL * HEAD_DIM, D), (HEAD_TOTAL * HEAD_DIM // 16) ** -0.5, 0.75, ((1, 16),))
    expert_rows = gaussian(streams_of[7], (TOKB, D), 1.0, 6.0, ((0, 32),))
    expert_gain = jnp.clip(1.0 + 0.18 * jax.random.normal(streams_of[8], (D,), jnp.float32), 0.1, 1.9)
    routes_keys = jax.random.split(jax.random.fold_in(streams_of[9], 1), TOKB // TOKB_DEV)
    routes_turns = jax.random.permutation(jax.random.fold_in(streams_of[9], 3), TOKB // TOKB_DEV)
    routes = jax.vmap(lambda own, number: shared_out(jax.random.fold_in(streams_of[9], 2), own, number, TOKB_DEV, EXPERTS, TOPK, CAP, 2))(routes_keys, routes_turns).reshape((TOKB, TOPK))
    route_weight = jnp.clip(0.05 + 0.55 * jax.random.uniform(streams_of[10], (TOKB, TOPK), jnp.float32) ** steps_of(streams_of[10], (TOKB, TOPK), ((0, 32),), -0.2, 0.2), 0.05, 0.6)
    w_gate = gaussian(streams_of[11], (EXPERTS, D, FF), (D // 4) ** -0.5, 0.25, ((0, 32), (2, 16)))
    w_up = gaussian(streams_of[12], (EXPERTS, D, FF), (D // 4) ** -0.5, 0.25, ((0, 32), (2, 16)))
    w_down = gaussian(streams_of[13], (EXPERTS, FF, D), (4 * FF) ** -0.5, 0.0625, ((0, 32), (2, 16)))
    return {"mixer_rows": mixer_rows, "mixer_gain": mixer_gain, "w_query": w_query, "w_key": w_key, "w_value": w_value, "key_shift": key_shift, "w_out": w_out, "expert_rows": expert_rows, "expert_gain": expert_gain, "routes": routes, "route_weight": route_weight, "w_gate": w_gate, "w_up": w_up, "w_down": w_down}


norm_eps = 1e-06
glu_limit = 7.0
glu_alpha = 1.702

def rms_scale(source, scaling):
    floats = source.astype(jnp.float32)
    inverse = lax.rsqrt(lax.optimization_barrier(jnp.mean(floats * floats, axis=-1, keepdims=True)) + norm_eps)
    return (floats * inverse * scaling).astype(jnp.bfloat16)

def mixer_layer(mixer_rows, mixer_gain, w_query, w_key, w_value, key_shift, w_out):
    normed = rms_scale(mixer_rows, mixer_gain)
    total_rows = normed.shape[0]

    def project(weight):
        flat_out = jnp.dot(normed, weight, preferred_element_type=jnp.float32).astype(jnp.bfloat16)
        return flat_out.reshape(total_rows, HEAD_TOTAL, HEAD_DIM).transpose(1, 0, 2)
    positions = jnp.arange(total_rows, dtype=jnp.int32)
    block_starts = jnp.arange(total_rows // TOKA_DEV, dtype=jnp.int32) * TOKA_DEV

    def one_head(operands):
        query_head, key_head, value_head, shift_head = operands

        def one_block(begin_at):
            query_block = lax.dynamic_slice_in_dim(query_head, begin_at, TOKA_DEV, 0)
            query_pos = begin_at + jnp.arange(TOKA_DEV, dtype=jnp.int32)
            strict = positions[None, :] < query_pos[:, None]
            scores = jnp.dot(query_block, key_head.T, preferred_element_type=jnp.float32) * HEAD_DIM ** (-0.5)
            scores = scores + shift_head[None, :]
            log_stay = jnp.where(strict, jax.nn.log_sigmoid(-scores), 0.0)
            between = lax.cumsum(log_stay, axis=1, reverse=True) - log_stay
            weights = jnp.where(strict, jnp.exp(jax.nn.log_sigmoid(scores) + between), 0.0).astype(jnp.bfloat16)
            return jnp.dot(weights, value_head, preferred_element_type=jnp.float32).astype(jnp.bfloat16)
        return lax.map(one_block, block_starts).reshape(total_rows, HEAD_DIM)
    heads_out = lax.map(one_head, (project(w_query), project(w_key), project(w_value), key_shift))
    head_out = heads_out.transpose(1, 0, 2).reshape(total_rows, HEAD_TOTAL * HEAD_DIM)
    return jnp.dot(head_out, w_out, preferred_element_type=jnp.float32).astype(jnp.bfloat16)

def expert_layer(expert_rows, expert_gain, routes, route_weight, w_gate, w_up, w_down):
    normed = rms_scale(expert_rows, expert_gain)
    tokens_all = normed.shape[0]
    chosen = routes.reshape(-1).astype(jnp.int32)
    hit_table = (chosen[:, None] == jnp.arange(EXPERTS, dtype=jnp.int32)[None, :]).astype(jnp.int32)
    places = lax.optimization_barrier(jnp.sum((jnp.cumsum(hit_table, axis=0) - 1) * hit_table, axis=1)).astype(jnp.int32)
    room_size = N_EP * CAP
    targets = chosen * room_size + places
    assign_ids = jnp.arange(tokens_all * TOPK, dtype=jnp.int32) // TOPK
    owners = jnp.full((EXPERTS * room_size,), tokens_all, jnp.int32).at[targets].set(assign_ids)
    padded = jnp.concatenate([normed, jnp.zeros((1, D), jnp.bfloat16)], axis=0)

    def one_expert(operands):
        slot_ids, gate_cols, upper_cols, down_rows = operands
        picked_rows = padded[slot_ids]
        gating = jnp.minimum(jnp.dot(picked_rows, gate_cols, preferred_element_type=jnp.float32), glu_limit)
        linear = jnp.clip(jnp.dot(picked_rows, upper_cols, preferred_element_type=jnp.float32), -glu_limit, glu_limit)
        hidden = (gating * jax.nn.sigmoid(glu_alpha * gating) * (linear + 1.0)).astype(jnp.bfloat16)
        return jnp.dot(hidden, down_rows, preferred_element_type=jnp.float32).astype(jnp.bfloat16)
    results = lax.map(one_expert, (owners.reshape(EXPERTS, room_size), w_gate, w_up, w_down))
    picked = results.reshape(EXPERTS * room_size, D)[targets].astype(jnp.float32) * route_weight.reshape(-1)[:, None]
    return lax.optimization_barrier(jnp.sum(picked.reshape(tokens_all, TOPK, D), axis=1)).astype(jnp.bfloat16)

def reference(mixer_rows, mixer_gain, w_query, w_key, w_value, key_shift, w_out, expert_rows, expert_gain, routes, route_weight, w_gate, w_up, w_down):
    mixer_out = mixer_layer(mixer_rows, mixer_gain, w_query, w_key, w_value, key_shift, w_out)
    expert_out = expert_layer(expert_rows, expert_gain, routes, route_weight, w_gate, w_up, w_down)
    return (mixer_out, expert_out)
```

```python
import jax
import jax.numpy as jnp
from jax import lax
from jax.sharding import Mesh
from jax.experimental import pallas as pl
from jax.experimental.pallas import tpu as pltpu
from jax.sharding import PartitionSpec as P

EP = ("ep_0", "ep_1")


norm_eps = 1e-06
glu_limit = 7.0
glu_alpha = 1.702


def in_order(blocks, dim):
    shape = list(blocks.shape[1:])
    shape[dim] *= blocks.shape[0]
    return jnp.moveaxis(blocks, 0, dim).reshape(shape)


def all_blocks(shard, axes, turns):
    blocks = shard[None]
    for k in turns:
        blocks = lax.all_gather(blocks, axes[k], axis=0, tiled=True)
    carried = [lax.axis_size(axes[k]) for k in reversed(turns)]
    blocks = blocks.reshape(*carried, *shard.shape)
    turned = sorted(range(len(turns)), key=lambda place: turns[len(turns) - 1 - place])
    return blocks.transpose(*turned, *range(len(turns), blocks.ndim)).reshape(-1, *shard.shape)


def whole_of(shard, axes, turns, dim):
    return in_order(all_blocks(shard, axes, turns), dim)


def copy_for_each(shard, axis):
    devices = lax.axis_size(axis)
    return lax.all_to_all(
        jnp.broadcast_to(shard[None], (devices, *shard.shape)), axis, 0, 0, tiled=True
    )


def gather_directly(shard, axis, dim):
    blocks = copy_for_each(shard, axis)
    return in_order(blocks, dim)


def rms_scale(source, scaling):
    floats = source.astype(jnp.float32)
    inverse = lax.rsqrt(jnp.mean(floats * floats, axis=-1, keepdims=True) + norm_eps)
    return (floats * inverse * scaling).astype(jnp.bfloat16)


def stick_step(query, keyed, valued, shifting, triangle, carried, allowed):
    scores = lax.dot_general(
        query, keyed, (((1,), (1,)), ((), ())), preferred_element_type=jnp.float32
    )
    scores = scores + shifting
    tail = jnp.log(1.0 + jnp.exp(-jnp.abs(scores)))
    soft = jnp.maximum(scores, 0.0) + tail
    if allowed is not None:
        soft = jnp.where(allowed, soft, 0.0)
    high = soft.astype(jnp.bfloat16)
    low = (soft - high.astype(jnp.float32)).astype(jnp.bfloat16)
    after = jnp.dot(high, triangle, preferred_element_type=jnp.float32)
    after = after + jnp.dot(low, triangle, preferred_element_type=jnp.float32)
    weights = jnp.exp(jnp.minimum(scores, 0.0) - tail - (after + carried))
    if allowed is not None:
        weights = jnp.where(allowed, weights, 0.0)
    contrib = jnp.dot(weights.astype(jnp.bfloat16), valued, preferred_element_type=jnp.float32)
    return contrib, carried + after[:, :1] + soft[:, :1]


def stick_kernel(query_ref, packed_ref, shift_ref, out_ref):
    device = lax.axis_index(EP)
    length, head_width = query_ref.shape
    query = query_ref[...] * jnp.bfloat16(head_width ** (-0.5))
    rows = lax.broadcasted_iota(jnp.int32, (length, length), 0)
    cols = lax.broadcasted_iota(jnp.int32, (length, length), 1)
    triangle = (rows > cols).astype(jnp.float32).astype(jnp.bfloat16)

    def block(anchor, carried, allowed):
        packed = packed_ref[anchor]
        return stick_step(
            query,
            packed[:, :head_width],
            packed[:, head_width:],
            shift_ref[anchor],
            triangle,
            carried,
            allowed,
        )

    summed, carried = block(device, jnp.zeros((length, 1), jnp.float32), cols < rows)

    def visiting(offset, status):
        running, carry_now = status
        contrib, carry_now = block(device - offset, carry_now, None)
        return running + contrib, carry_now

    summed, carried = lax.fori_loop(1, device + 1, visiting, (summed, carried))
    out_ref[...] = summed.astype(out_ref.dtype)


def per_device(
    mixer_rows,
    mixer_gain,
    w_query,
    w_key,
    w_value,
    key_shift,
    w_out,
    expert_rows,
    expert_gain,
    routes,
    route_weight,
    w_gate,
    w_up,
    w_down,
):
    length = mixer_rows.shape[0]
    head_count = key_shift.shape[0]
    head_width = w_query.shape[1] // head_count
    normed = rms_scale(mixer_rows, mixer_gain)
    queries = jnp.dot(normed, w_query, preferred_element_type=jnp.float32).astype(jnp.bfloat16)
    key_rows = jnp.dot(normed, w_key, preferred_element_type=jnp.float32).astype(jnp.bfloat16)
    value_rows = jnp.dot(normed, w_value, preferred_element_type=jnp.float32).astype(jnp.bfloat16)
    packed = jnp.concatenate([key_rows, value_rows], axis=1)
    gathered = all_blocks(packed, EP, (0, 1))
    head_out = pl.pallas_call(
        stick_kernel,
        out_shape=jax.ShapeDtypeStruct((length, head_width), jnp.bfloat16),
        in_specs=[pl.BlockSpec(memory_space=pltpu.VMEM)] * 3,
        out_specs=pl.BlockSpec(memory_space=pltpu.VMEM),
    )(queries, gathered, key_shift.reshape(-1, 1, length))
    weight_rows = w_out
    mixer_out = jnp.dot(
        gather_directly(head_out, "tp", 1), weight_rows, preferred_element_type=jnp.float32
    ).astype(jnp.bfloat16)
    tokens_here, top_count = routes.shape
    expert_count = lax.axis_size(EP)
    capacity = 2 * tokens_here * top_count // expert_count
    rows_after_norm = rms_scale(expert_rows, expert_gain)
    chosen = routes.reshape(-1)
    hit_table = (chosen[:, None] == jnp.arange(expert_count, dtype=jnp.int32)[None, :]).astype(
        jnp.int32
    )
    places = jnp.sum((jnp.cumsum(hit_table, axis=0) - 1) * hit_table, axis=1)
    targets = chosen * capacity + places
    assign_ids = jnp.arange(tokens_here * top_count, dtype=jnp.int32) // top_count
    owners = (
        jnp.full((expert_count * capacity,), tokens_here, jnp.int32).at[targets].set(assign_ids)
    )
    padded = jnp.concatenate(
        [rows_after_norm, jnp.zeros((1, rows_after_norm.shape[1]), jnp.bfloat16)], axis=0
    )
    outgoing = padded[owners].reshape(expert_count, capacity, rows_after_norm.shape[1])
    gate_cols = w_gate[0]
    upper_cols = w_up[0]
    down_rows = w_down[0]
    portion_size = capacity // lax.axis_size("tp")
    own_slots = lax.dynamic_slice_in_dim(
        outgoing, lax.axis_index("tp") * portion_size, portion_size, 1
    )
    arrived = lax.all_to_all(own_slots, EP, split_axis=0, concat_axis=0, tiled=True)
    expert_arrived = lax.all_gather(arrived, "tp", axis=1, tiled=True)
    expert_senders, slots_here, feature_count = expert_arrived.shape
    flat_rows = expert_arrived.reshape(expert_senders * slots_here, feature_count)
    gating = jnp.minimum(
        jnp.dot(flat_rows, gate_cols, preferred_element_type=jnp.float32), glu_limit
    )
    linear = jnp.clip(
        jnp.dot(flat_rows, upper_cols, preferred_element_type=jnp.float32), -glu_limit, glu_limit
    )
    hidden = gating * jax.nn.sigmoid(glu_alpha * gating) * (linear + 1.0)
    hidden = hidden.astype(jnp.bfloat16).reshape(expert_senders, slots_here, gate_cols.shape[1])
    senders = hidden.shape[0]
    slot_total = hidden.shape[1]
    portion_units = lax.all_gather(hidden, "tp", axis=2, tiled=True)
    weight_rows = down_rows
    flat_units = portion_units.reshape(senders * slot_total, portion_units.shape[2])
    results = jnp.dot(flat_units, weight_rows, preferred_element_type=jnp.float32)
    leaving = results.astype(jnp.bfloat16).reshape(senders, slot_total, down_rows.shape[1])
    returned = lax.all_to_all(leaving, EP, split_axis=0, concat_axis=0, tiled=True)
    picked = returned.reshape(expert_count * capacity, down_rows.shape[1])[targets].astype(
        jnp.float32
    )
    picked = picked * route_weight.reshape(-1)[:, None]
    expert_out = jnp.sum(picked.reshape(tokens_here, top_count, down_rows.shape[1]), axis=1).astype(
        jnp.bfloat16
    )
    return (mixer_out, expert_out)


def solution(mesh):
    torus = Mesh(mesh.devices.reshape(16, 2, mesh.shape["tp"]), ("ep_0", "ep_1", "tp"))
    return jax.shard_map(
        per_device,
        mesh=torus,
        in_specs=(
            P(EP, None),
            P(),
            P(None, "tp"),
            P(None, "tp"),
            P(None, "tp"),
            P("tp", None),
            P(None, "tp"),
            P(EP, None),
            P(),
            P(EP, None),
            P(EP, None),
            P(EP, None, "tp"),
            P(EP, None, "tp"),
            P(EP, None, "tp"),
        ),
        out_specs=(P(EP, "tp"), P(EP, "tp")),
        check_vma=False,
    )
```

```python
import jax
import jax.numpy as jnp
from jax import lax
from jax.experimental import pallas as pl
from jax.experimental.pallas import tpu as pltpu
from jax.sharding import Mesh
from jax.sharding import PartitionSpec as P

MESH = pl.DeviceIdType.MESH
EP = ("z", "c")
TP = ("y", "x")
BF = jnp.bfloat16
F32 = jnp.float32

norm_eps = 1e-06
glu_limit = 7.0
glu_alpha = 1.702

SHIFT_Z = 3


def iota(shape, dim):
    return lax.broadcasted_iota(jnp.int32, shape, dim)


def rms_scale(source, scaling):
    floats = source.astype(F32)
    inverse = lax.rsqrt(jnp.mean(floats * floats, axis=-1, keepdims=True) + norm_eps)
    return (floats * inverse * scaling).astype(BF)


def split_three(value):
    high = value.astype(BF)
    rest = value - high.astype(F32)
    middle = rest.astype(BF)
    low = (rest - middle.astype(F32)).astype(BF)
    return high, middle, low


def before_kernel(
    rows_ref,
    gain_ref,
    wq_ref,
    wk_ref,
    wv_ref,
    tokens_ref,
    token_gain_ref,
    routes_ref,
    weight_ref,
    query_ref,
    packed_ref,
    outgoing_ref,
    combine_ref,
    picked,
):
    length, width = rows_ref.shape
    head = wq_ref.shape[1]
    normed = rms_scale(rows_ref[...], gain_ref[...])
    query = jnp.dot(normed, wq_ref[...], preferred_element_type=F32).astype(BF)
    query_ref[...] = query * BF(head ** (-0.5))
    packed_ref[:, :head] = jnp.dot(normed, wk_ref[...], preferred_element_type=F32).astype(BF)
    packed_ref[:, head:] = jnp.dot(normed, wv_ref[...], preferred_element_type=F32).astype(BF)

    tokens, top = routes_ref.shape
    experts = outgoing_ref.shape[0]
    cap = combine_ref.shape[2] // experts
    part = lax.axis_index("y") * lax.axis_size("x") + lax.axis_index("x")
    normed_b = rms_scale(tokens_ref[...], token_gain_ref[...])
    chosen = routes_ref[...]
    lanes = iota((tokens, experts), 1)
    hits = jnp.zeros((tokens, experts), F32)
    for k in range(top):
        hits = hits + (chosen[:, k : k + 1] == lanes).astype(F32)
    earlier = (iota((tokens, tokens), 1) < iota((tokens, tokens), 0)).astype(F32).astype(BF)
    places = jnp.dot(earlier, hits.astype(BF), preferred_element_type=F32)
    slots = iota((tokens, experts * 2), 1)
    spots = iota((tokens, experts * cap), 1)
    select = jnp.zeros((tokens, experts * 2), F32)
    combine = jnp.zeros((tokens, experts * cap), F32)
    for k in range(top):
        expert = chosen[:, k : k + 1]
        place = jnp.sum(jnp.where(expert == lanes, places, 0.0), axis=1, keepdims=True)
        place = place.astype(jnp.int32)
        own = place - 2 * part
        wanted = jnp.where((own >= 0) & (own < 2), expert * 2 + own, -1)
        select = select + (wanted == slots).astype(F32)
        combine = combine + jnp.where(
            expert * cap + place == spots, weight_ref[:, k : k + 1], 0.0
        )
    picked[...] = lax.dot_general(
        select.astype(BF), normed_b, (((0,), (0,)), ((), ())), preferred_element_type=F32
    ).astype(BF)
    for e in range(experts):
        outgoing_ref[e] = picked[2 * e : 2 * e + 2, :]
    for n, term in enumerate(split_three(combine)):
        combine_ref[n] = term


class Plane:
    def __init__(self, piece, recv, send, here):
        self.piece, self.recv, self.send, self.here = piece, recv, send, here
        self.started = []
        self.used = [0, 0]

    def descriptor(self, part, off, axis, delta):
        x, y = self.here["x"], self.here["y"]
        slot = lax.rem(y + off["y"] + 4, 4) * 4 + lax.rem(x + off["x"] + 4, 4)
        there = dict(off)
        there[axis] -= delta
        index = (there["y"] % 4) * 4 + there["x"] % 4
        ref = self.piece(slot, part)
        number = self.used[part]
        return pltpu.make_async_remote_copy(
            src_ref=ref,
            dst_ref=ref,
            send_sem=self.send.at[part, min(number, 15)],
            recv_sem=self.recv.at[part, index],
            device_id={axis: lax.rem(self.here[axis] + delta + 4, 4)},
            device_id_type=MESH,
        )

    def put(self, part, off, axis, delta):
        copy = self.descriptor(part, off, axis, delta)
        copy.start()
        self.used[part] += 1
        self.started.append(copy)

    def take(self, part, off, axis, delta):
        x, y = self.here["x"], self.here["y"]
        slot = lax.rem(y + off["y"] + 4, 4) * 4 + lax.rem(x + off["x"] + 4, 4)
        ref = self.piece(slot, part)
        index = (off["y"] % 4) * 4 + off["x"] % 4
        pltpu.make_async_remote_copy(
            src_ref=ref,
            dst_ref=ref,
            send_sem=self.send.at[part, 15],
            recv_sem=self.recv.at[part, index],
            device_id={axis: lax.rem(self.here[axis] - delta + 4, 4)},
            device_id_type=MESH,
        ).wait_recv()

    AXES = (("x", "y"), ("y", "x"))

    @staticmethod
    def at(axes, f, s):
        return {axes[0]: f, axes[1]: s}

    def stage0(self):
        for part, axes in enumerate(self.AXES):
            for delta in (1, -1):
                self.put(part, self.at(axes, 0, 0), axes[0], delta)
        for part, axes in enumerate(self.AXES):
            for delta in (1, -1):
                self.put(part, self.at(axes, 0, 0), axes[1], delta)

    def spread(self, part, axes, f):
        for delta in (1, -1):
            self.put(part, self.at(axes, f, 0), axes[1], delta)

    def stage1(self):
        for part, axes in enumerate(self.AXES):
            self.take(part, self.at(axes, -1, 0), axes[0], 1)
            self.put(part, self.at(axes, -1, 0), axes[0], 1)
            self.spread(part, axes, -1)
        for part, axes in enumerate(self.AXES):
            self.take(part, self.at(axes, 1, 0), axes[0], -1)
            self.spread(part, axes, 1)

    def stage2(self):
        for part, axes in enumerate(self.AXES):
            self.take(part, self.at(axes, 2, 0), axes[0], 1)
            self.spread(part, axes, 2)

    def stage3(self):
        for f in (0, -1, 1, 2):
            sign = 1 if f in (0, 1) else -1
            for part, axes in enumerate(self.AXES):
                self.take(part, self.at(axes, f, -sign), axes[1], sign)
                self.put(part, self.at(axes, f, -sign), axes[1], sign)
            for part, axes in enumerate(self.AXES):
                self.take(part, self.at(axes, f, sign), axes[1], -sign)

    def stage4(self):
        for f in (0, -1, 1, 2):
            sign = 1 if f in (0, 1) else -1
            for part, axes in enumerate(self.AXES):
                self.take(part, self.at(axes, f, 2), axes[1], sign)

    def finish(self):
        for copy in self.started:
            copy.wait_send()


def main_kernel(
    query_ref,
    packed_ref,
    shift_ref,
    outgoing_ref,
    combine_ref,
    gate_ref,
    up_ref,
    down_ref,
    out_ref,
    mixer_ref,
    expert_ref,
    arrived,
    rows,
    hidden,
    leaving,
    returned,
    kv,
    heads,
    running,
    carry,
    sent_recv,
    sent_send,
    plane_recv,
    plane_send,
    kv_recv,
    kv_send,
    head_recv,
    head_send,
    back_recv,
    back_send,
):
    nz = lax.axis_size("z")
    z, c = lax.axis_index("z"), lax.axis_index("c")
    y, x = lax.axis_index("y"), lax.axis_index("x")
    here = {"x": x, "y": y}
    part = y * 4 + x
    device = z * 2 + c
    half_z = nz // 2
    started = []

    def at_z(delta):
        return lax.rem(z + delta + nz, nz)

    barrier = pltpu.get_barrier_semaphore()
    peers = 0
    for dz in range(nz):
        for k in range(2):
            if dz or k:
                pl.semaphore_signal(
                    barrier,
                    inc=1,
                    device_id={"z": at_z(dz), "c": lax.rem(c + k, 2)},
                    device_id_type=MESH,
                )
                peers += 1
    for oy in range(4):
        for ox in range(4):
            if oy or ox:
                pl.semaphore_signal(
                    barrier,
                    inc=1,
                    device_id={"y": lax.rem(y + oy, 4), "x": lax.rem(x + ox, 4)},
                    device_id_type=MESH,
                )
                peers += 1
    pl.semaphore_wait(barrier, peers)

    def dispatch(o, k):
        zt, ct = at_z(SHIFT_Z - o), lax.rem(c + k, 2)
        return pltpu.make_async_remote_copy(
            src_ref=outgoing_ref.at[zt * 2 + ct],
            dst_ref=arrived.at[o * 2 + c],
            send_sem=sent_send.at[o * 2 + k],
            recv_sem=sent_recv.at[o * 2 + k],
            device_id={"z": zt, "c": ct},
            device_id_type=MESH,
        )

    order = sorted(range(nz), key=lambda o: (o >= half_z, -abs(SHIFT_Z - o)))
    for o in order:
        for k in range(2):
            if o == SHIFT_Z and k == 0:
                continue
            copy = dispatch(o, k)
            copy.start()
            started.append(copy)
    arrived[SHIFT_Z * 2 + c] = outgoing_ref[device]

    def pass_on(block, src, index, target):
        copy = pltpu.make_async_remote_copy(
            src_ref=src,
            dst_ref=kv.at[block],
            send_sem=kv_send.at[index],
            recv_sem=kv_recv.at[index],
            device_id=target,
            device_id_type=MESH,
        )
        copy.start()
        started.append(copy)

    def got(block, index):
        pltpu.make_async_remote_copy(
            src_ref=kv.at[block],
            dst_ref=kv.at[block],
            send_sem=kv_send.at[index],
            recv_sem=kv_recv.at[index],
            device_id={"c": 1 - c},
            device_id_type=MESH,
        ).wait_recv()

    ups, downs = half_z, half_z - 1
    up0, down0, pup0, pdown0 = 0, ups, 2 * half_z, 3 * half_z + 1

    def ring(step):
        if step == 0:
            pass_on(device, packed_ref, up0, {"z": at_z(1)})
            pass_on(device, packed_ref, down0, {"z": at_z(-1)})
            pass_on(device, packed_ref, pup0, {"c": 1 - c})
            kv[device] = packed_ref[...]
            return
        block = at_z(-step) * 2 + c
        got(block, up0 + step - 1)
        if step < ups:
            pass_on(block, kv.at[block], up0 + step, {"z": at_z(1)})
        pass_on(block, kv.at[block], pup0 + step, {"c": 1 - c})
        if step <= downs:
            block = at_z(step) * 2 + c
            got(block, down0 + step - 1)
            if step < downs:
                pass_on(block, kv.at[block], down0 + step, {"z": at_z(-1)})
            pass_on(block, kv.at[block], pdown0 + step - 1, {"c": 1 - c})

    def partner_up(step):
        got(at_z(-step) * 2 + 1 - c, pup0 + step)

    def partner_down(step):
        got(at_z(step) * 2 + 1 - c, pdown0 + step - 1)

    length, head = query_ref.shape

    def stick(anchor, diagonal):
        packed = kv[anchor]
        scores = lax.dot_general(
            query_ref[...],
            packed[:, :head],
            (((1,), (1,)), ((), ())),
            preferred_element_type=F32,
        )
        scores = scores + shift_ref[anchor]
        tail = jnp.log(1.0 + jnp.exp(-jnp.abs(scores)))
        soft = jnp.maximum(scores, 0.0) + tail
        square = (length, length)
        if diagonal:
            allowed = iota(square, 1) < iota(square, 0)
            soft = jnp.where(allowed, soft, 0.0)
        triangle = (iota(square, 0) > iota(square, 1)).astype(F32).astype(BF)
        high = soft.astype(BF)
        low = (soft - high.astype(F32)).astype(BF)
        after = jnp.dot(high, triangle, preferred_element_type=F32)
        after = after + jnp.dot(low, triangle, preferred_element_type=F32)
        before = 0.0 if diagonal else carry[...]
        weights = jnp.exp(jnp.minimum(scores, 0.0) - tail - (after + before))
        if diagonal:
            weights = jnp.where(allowed, weights, 0.0)
        contrib = jnp.dot(weights.astype(BF), packed[:, head:], preferred_element_type=F32)
        total = after[:, :1] + soft[:, :1]
        if diagonal:
            running[...] = contrib
            carry[...] = total
        else:
            running[...] += contrib
            carry[...] += total

    def attend(first, last):
        low = 1 if first == 0 else 2 * first - 1 + c
        high = jnp.minimum(2 * last + c, device)

        def one(offset, none):
            stick(device - offset, False)
            return none

        lax.fori_loop(low, high + 1, one, 0)

    def gathering(number, piece):
        return Plane(piece, plane_recv.at[number], plane_send.at[number], here)

    gathers = [
        gathering(0, lambda slot, half: rows.at[0, slot * 2 + half]),
        gathering(1, lambda slot, half: rows.at[1, slot * 2 + half]),
        gathering(2, lambda slot, half: hidden.at[0, slot * 2 + half]),
        gathering(3, lambda slot, half: hidden.at[1, slot * 2 + half]),
    ]
    rows0, rows1, hidden0, hidden1 = gathers

    def lay_out(group):
        for o in range(group * half_z, (group + 1) * half_z):
            for k in range(2):
                if o == SHIFT_Z and k == 0:
                    continue
                zs, cs = at_z(o - SHIFT_Z), lax.rem(c + k, 2)
                pltpu.make_async_remote_copy(
                    src_ref=outgoing_ref.at[zs * 2 + cs],
                    dst_ref=arrived.at[o * 2 + cs],
                    send_sem=sent_send.at[o * 2 + k],
                    recv_sem=sent_recv.at[o * 2 + k],
                    device_id={"z": zs, "c": cs},
                    device_id_type=MESH,
                ).wait_recv()
        for n in range(nz):
            half, line = divmod(n, half_z)
            rows[group, part * 2 + half, 2 * line : 2 * line + 2, :] = arrived[group * nz + n]

    def expand(group):
        both = jnp.concatenate([gate_ref[...], up_ref[...]], axis=1)
        units = gate_ref.shape[1]

        def one(n, none):
            block = rows[group, pl.ds(n * 8, 8)].reshape(128, -1)
            flat = jnp.dot(block, both, preferred_element_type=F32)
            gating = jnp.minimum(flat[:, :units], glu_limit)
            linear = jnp.clip(flat[:, units:], -glu_limit, glu_limit)
            value = gating * jax.nn.sigmoid(glu_alpha * gating) * (linear + 1.0)
            where = pl.multiple_of(lax.rem(n, 2) * 128, 128)
            hidden[group, part * 2 + n // 2, pl.ds(where, 128), :] = value.astype(BF)
            return none

        lax.fori_loop(0, 4, one, 0)

    def contract(group):
        total = 512
        results = []
        for half in range(2):
            result = jnp.zeros((256, 128), F32)
            for pair in range(8):
                units = jnp.concatenate(
                    [hidden[group, 4 * pair + half], hidden[group, 4 * pair + 2 + half]], axis=1
                )
                result = result + jnp.dot(
                    units, down_ref[pair * 256 : (pair + 1) * 256], preferred_element_type=F32
                )
            results.append(result.astype(BF))
        stacked = jnp.concatenate(results, axis=0)
        to, of = iota((total, total), 0), iota((total, total), 1)
        source = ((to >> 1) & 15) * 32 + (to >> 5) * 2 + (to & 1)
        turned = jnp.dot(
            (source == of).astype(F32).astype(BF), stacked, preferred_element_type=F32
        ).astype(BF)
        leaving[group] = turned.reshape(nz, 32, 128)

    def send_back(o, k):
        zt, ct = at_z(o - SHIFT_Z), lax.rem(c + k, 2)
        group, line = divmod(o, half_z)
        return pltpu.make_async_remote_copy(
            src_ref=leaving.at[group, line * 2 + ct],
            dst_ref=returned.at[device],
            send_sem=back_send.at[o * 2 + k],
            recv_sem=back_recv.at[o * 2 + k],
            device_id={"z": zt, "c": ct},
            device_id_type=MESH,
        )

    def give_back(group):
        for o in order:
            if o // half_z != group:
                continue
            for k in range(2):
                if o == SHIFT_Z and k == 0:
                    continue
                copy = send_back(o, k)
                copy.start()
                started.append(copy)
        if group == 0:
            returned[device] = leaving[0, SHIFT_Z * 2 + c]

    def head_copy(oy, ox):
        index = ((-oy) % 4) * 4 + (-ox) % 4
        return pltpu.make_async_remote_copy(
            src_ref=heads.at[part],
            dst_ref=heads.at[part],
            send_sem=head_send.at[oy * 4 + ox],
            recv_sem=head_recv.at[index],
            device_id={"y": lax.rem(y + oy, 4), "x": lax.rem(x + ox, 4)},
            device_id_type=MESH,
        )

    def head_wait(oy, ox):
        slot = lax.rem(y + oy, 4) * 4 + lax.rem(x + ox, 4)
        pltpu.make_async_remote_copy(
            src_ref=heads.at[slot],
            dst_ref=heads.at[slot],
            send_sem=head_send.at[oy * 4 + ox],
            recv_sem=head_recv.at[oy * 4 + ox],
            device_id={"y": lax.rem(y + oy, 4), "x": lax.rem(x + ox, 4)},
            device_id_type=MESH,
        ).wait_recv()

    ring(0)
    stick(device, True)
    lay_out(0)
    rows0.stage0()
    ring(1)
    rows0.stage1()
    rows0.stage2()
    lay_out(1)
    rows1.stage0()
    ring(2)
    partner_up(0)
    partner_up(1)
    attend(0, 1)
    rows0.stage3()
    ring(3)
    rows1.stage1()
    ring(4)
    partner_up(2)
    partner_up(3)
    attend(2, 3)
    rows0.stage4()
    expand(0)
    ring(5)
    hidden0.stage0()
    rows1.stage2()
    ring(6)
    rows1.stage3()
    hidden0.stage1()
    ring(7)
    partner_up(4)
    partner_up(5)
    partner_up(6)
    attend(4, 6)
    ring(8)
    rows1.stage4()
    expand(1)
    hidden0.stage2()
    hidden1.stage0()
    hidden0.stage3()
    partner_up(7)
    partner_up(8)
    for step in range(1, downs + 1):
        partner_down(step)
    attend(7, 10)
    hidden1.stage1()
    hidden0.stage4()
    contract(0)
    hidden1.stage2()
    give_back(0)
    attend(11, nz - 1)
    hidden1.stage3()
    summed = running[...].astype(BF)
    heads[part, :, :head] = summed[: length // 2]
    heads[part, :, head:] = summed[length // 2 :]
    hidden1.stage4()
    for oy in range(4):
        for ox in range(4):
            if oy or ox:
                copy = head_copy(oy, ox)
                copy.start()
                started.append(copy)
    contract(1)
    give_back(1)
    for oy in range(4):
        for ox in range(4):
            if oy or ox:
                head_wait(oy, ox)

    mixed = jnp.zeros((length, 128), F32)
    for n in range(16):
        pair = heads[n]
        lines = jnp.concatenate([pair[:, :head], pair[:, head:]], axis=0)
        mixed = mixed + jnp.dot(
            lines, out_ref[n * head : (n + 1) * head], preferred_element_type=F32
        )
    mixer_ref[...] = mixed.astype(BF)

    for o in range(nz):
        for k in range(2):
            if o == SHIFT_Z and k == 0:
                continue
            zt, ct = at_z(SHIFT_Z - o), lax.rem(c + k, 2)
            pltpu.make_async_remote_copy(
                src_ref=returned.at[zt * 2 + ct],
                dst_ref=returned.at[zt * 2 + ct],
                send_sem=back_send.at[o * 2 + k],
                recv_sem=back_recv.at[o * 2 + k],
                device_id={"z": zt, "c": ct},
                device_id_type=MESH,
            ).wait_recv()
    table = returned[...].reshape(-1, 128)
    final = jnp.dot(combine_ref[0], table, preferred_element_type=F32)
    for n in range(1, 3):
        final = final + jnp.dot(combine_ref[n], table, preferred_element_type=F32)
    expert_ref[...] = final.astype(BF)

    for copy in started:
        copy.wait_send()
    for gather in gathers:
        gather.finish()


def per_device(
    mixer_rows,
    mixer_gain,
    w_query,
    w_key,
    w_value,
    key_shift,
    w_out,
    expert_rows,
    expert_gain,
    routes,
    route_weight,
    w_gate,
    w_up,
    w_down,
):
    length, width = mixer_rows.shape
    head = w_query.shape[1]
    tokens = expert_rows.shape[0]
    blocks = lax.axis_size("z") * 2
    cap = 2 * lax.axis_size("y") * lax.axis_size("x")
    vmem = pl.BlockSpec(memory_space=pltpu.VMEM)
    query, packed, outgoing, combine = pl.pallas_call(
        before_kernel,
        out_shape=(
            jax.ShapeDtypeStruct((length, head), BF),
            jax.ShapeDtypeStruct((length, 2 * head), BF),
            jax.ShapeDtypeStruct((blocks, 2, width), BF),
            jax.ShapeDtypeStruct((3, tokens, blocks * cap), BF),
        ),
        in_specs=[vmem] * 9,
        out_specs=(vmem,) * 4,
        scratch_shapes=[pltpu.VMEM((blocks * 2, width), BF)],
        name="before",
    )(
        mixer_rows,
        mixer_gain.reshape(1, -1),
        w_query,
        w_key,
        w_value,
        expert_rows,
        expert_gain.reshape(1, -1),
        routes,
        route_weight,
    )
    dma = pltpu.SemaphoreType.DMA
    return pl.pallas_call(
        main_kernel,
        out_shape=(
            jax.ShapeDtypeStruct((length, 128), BF),
            jax.ShapeDtypeStruct((tokens, 128), BF),
        ),
        in_specs=[vmem] * 9,
        out_specs=(vmem,) * 2,
        scratch_shapes=[
            pltpu.VMEM((blocks, 2, width), BF),
            pltpu.VMEM((2, 32, 16, width), BF),
            pltpu.VMEM((2, 32, 256, 128), BF),
            pltpu.VMEM((2, blocks // 2, 32, 128), BF),
            pltpu.VMEM((blocks, 32, 128), BF),
            pltpu.VMEM((blocks, length, 2 * head), BF),
            pltpu.VMEM((16, length // 2, 2 * head), BF),
            pltpu.VMEM((length, head), F32),
            pltpu.VMEM((length, 1), F32),
            dma((blocks,)),
            dma((blocks,)),
            dma((4, 2, 16)),
            dma((4, 2, 16)),
            dma((blocks,)),
            dma((blocks,)),
            dma((16,)),
            dma((16,)),
            dma((blocks,)),
            dma((blocks,)),
        ],
        compiler_params=pltpu.CompilerParams(
            collective_id=0, has_side_effects=True, vmem_limit_bytes=48 * 1024 * 1024
        ),
        name="main",
    )(
        query,
        packed,
        key_shift.reshape(-1, 1, length),
        outgoing,
        combine,
        w_gate[0],
        w_up[0],
        w_down[0],
        w_out,
    )


def solution(mesh):
    torus = Mesh(mesh.devices.reshape(16, 2, 4, 4), ("z", "c", "y", "x"))
    return jax.shard_map(
        per_device,
        mesh=torus,
        in_specs=(
            P(EP, None),
            P(),
            P(None, TP),
            P(None, TP),
            P(None, TP),
            P(TP, None),
            P(None, TP),
            P(EP, None),
            P(),
            P(EP, None),
            P(EP, None),
            P(EP, None, TP),
            P(EP, None, TP),
            P(EP, None, TP),
        ),
        out_specs=(P(EP, TP), P(EP, TP)),
        check_vma=False,
    )
```

```python
import jax
import jax.numpy as jnp
from jax import lax
from jax.experimental import pallas as pl
from jax.experimental.pallas import tpu as pltpu
from jax.sharding import Mesh
from jax.sharding import PartitionSpec as P

MESH = pl.DeviceIdType.MESH
EP = ("z", "c")
TP = ("y", "x")
BF = jnp.bfloat16
F32 = jnp.float32

norm_eps = 1e-06
glu_limit = 7.0
glu_alpha = 1.702

SHIFT_Z = 3


def iota(shape, dim):
    return lax.broadcasted_iota(jnp.int32, shape, dim)


def rms_scale(source, scaling):
    floats = source.astype(F32)
    inverse = lax.rsqrt(jnp.mean(floats * floats, axis=-1, keepdims=True) + norm_eps)
    return (floats * inverse * scaling).astype(BF)


def split_three(value):
    high = value.astype(BF)
    rest = value - high.astype(F32)
    middle = rest.astype(BF)
    low = (rest - middle.astype(F32)).astype(BF)
    return high, middle, low


def columns_of(routes, weights):
    top, tokens = routes.shape
    fill = jnp.zeros((128 - 2 * top, tokens), F32)
    stacked = jnp.concatenate([routes.astype(F32), weights, fill], axis=0)
    return jnp.transpose(stacked)


def places_of(table, top, experts):
    tokens = table.shape[0]
    lanes = iota((tokens, experts), 1).astype(F32)
    hits = jnp.zeros((tokens, experts), F32)
    for k in range(top):
        hits = hits + (table[:, k : k + 1] == lanes).astype(F32)
    earlier = (iota((tokens, tokens), 1) < iota((tokens, tokens), 0)).astype(F32).astype(BF)
    counts = jnp.dot(earlier, hits.astype(BF), preferred_element_type=F32)
    return [
        jnp.sum(jnp.where(table[:, k : k + 1] == lanes, counts, 0.0), axis=1, keepdims=True)
        for k in range(top)
    ]


def selection_of(table, places, top, experts, first):
    tokens = table.shape[0]
    slots = iota((tokens, experts * 2), 1).astype(F32)
    select = jnp.zeros((tokens, experts * 2), F32)
    for k in range(top):
        own = places[k] - first
        wanted = jnp.where((own >= 0.0) & (own < 2.0), table[:, k : k + 1] * 2.0 + own, -1.0)
        select = select + (wanted == slots).astype(F32)
    return select.astype(BF)


def combine_of(table, places, top, experts, cap):
    tokens = table.shape[0]
    spots = iota((tokens, experts * cap), 1).astype(F32)
    combine = jnp.zeros((tokens, experts * cap), F32)
    for k in range(top):
        spot = table[:, k : k + 1] * float(cap) + places[k]
        combine = combine + jnp.where(spot == spots, table[:, top + k : top + k + 1], 0.0)
    return split_three(combine)


class Plane:
    def __init__(self, piece, recv, send, here):
        self.piece, self.recv, self.send, self.here = piece, recv, send, here
        self.started = []
        self.used = [0, 0]

    def descriptor(self, part, off, axis, delta):
        x, y = self.here["x"], self.here["y"]
        slot = lax.rem(y + off["y"] + 4, 4) * 4 + lax.rem(x + off["x"] + 4, 4)
        there = dict(off)
        there[axis] -= delta
        index = (there["y"] % 4) * 4 + there["x"] % 4
        ref = self.piece(slot, part)
        number = self.used[part]
        return pltpu.make_async_remote_copy(
            src_ref=ref,
            dst_ref=ref,
            send_sem=self.send.at[part, min(number, 15)],
            recv_sem=self.recv.at[part, index],
            device_id={axis: lax.rem(self.here[axis] + delta + 4, 4)},
            device_id_type=MESH,
        )

    def put(self, part, off, axis, delta):
        copy = self.descriptor(part, off, axis, delta)
        copy.start()
        self.used[part] += 1
        self.started.append(copy)

    def take(self, part, off, axis, delta):
        x, y = self.here["x"], self.here["y"]
        slot = lax.rem(y + off["y"] + 4, 4) * 4 + lax.rem(x + off["x"] + 4, 4)
        ref = self.piece(slot, part)
        index = (off["y"] % 4) * 4 + off["x"] % 4
        pltpu.make_async_remote_copy(
            src_ref=ref,
            dst_ref=ref,
            send_sem=self.send.at[part, 15],
            recv_sem=self.recv.at[part, index],
            device_id={axis: lax.rem(self.here[axis] - delta + 4, 4)},
            device_id_type=MESH,
        ).wait_recv()

    AXES = (("x", "y"), ("y", "x"))

    @staticmethod
    def at(axes, f, s):
        return {axes[0]: f, axes[1]: s}

    def stage0(self):
        for part, axes in enumerate(self.AXES):
            for delta in (1, -1):
                self.put(part, self.at(axes, 0, 0), axes[0], delta)
        for part, axes in enumerate(self.AXES):
            for delta in (1, -1):
                self.put(part, self.at(axes, 0, 0), axes[1], delta)

    def spread(self, part, axes, f):
        for delta in (1, -1):
            self.put(part, self.at(axes, f, 0), axes[1], delta)

    def stage1(self):
        for part, axes in enumerate(self.AXES):
            self.take(part, self.at(axes, -1, 0), axes[0], 1)
            self.put(part, self.at(axes, -1, 0), axes[0], 1)
            self.spread(part, axes, -1)
        for part, axes in enumerate(self.AXES):
            self.take(part, self.at(axes, 1, 0), axes[0], -1)
            self.spread(part, axes, 1)

    def stage2(self):
        for part, axes in enumerate(self.AXES):
            self.take(part, self.at(axes, 2, 0), axes[0], 1)
            self.spread(part, axes, 2)

    def stage3(self):
        for f in (0, -1, 1, 2):
            sign = 1 if f in (0, 1) else -1
            for part, axes in enumerate(self.AXES):
                self.take(part, self.at(axes, f, -sign), axes[1], sign)
                self.put(part, self.at(axes, f, -sign), axes[1], sign)
            for part, axes in enumerate(self.AXES):
                self.take(part, self.at(axes, f, sign), axes[1], -sign)

    def stage4(self):
        for f in (0, -1, 1, 2):
            sign = 1 if f in (0, 1) else -1
            for part, axes in enumerate(self.AXES):
                self.take(part, self.at(axes, f, 2), axes[1], sign)

    def finish(self):
        for copy in self.started:
            copy.wait_send()


def main_kernel(
    rows_hbm,
    gain_ref,
    wq_hbm,
    wk_hbm,
    wv_hbm,
    shift_ref,
    out_hbm,
    tokens_hbm,
    token_gain_ref,
    routes_ref,
    weight_ref,
    gate_hbm,
    up_hbm,
    down_hbm,
    mixer_ref,
    expert_ref,
    source_ref,
    wq_ref,
    wk_ref,
    wv_ref,
    out_ref,
    tokens_ref,
    gate_ref,
    up_ref,
    down_ref,
    query_ref,
    packed_ref,
    picked,
    outgoing_ref,
    combine_ref,
    triangle_ref,
    arrived,
    rows,
    hidden,
    leaving,
    returned,
    kv,
    heads,
    running,
    carry,
    load_sem,
    sent_recv,
    sent_send,
    plane_recv,
    plane_send,
    kv_recv,
    kv_send,
    head_recv,
    head_send,
    back_recv,
    back_send,
):
    loads = {}
    for n, (name, src, dst) in enumerate(
        (
            ("tokens", tokens_hbm, tokens_ref),
            ("rows", rows_hbm, source_ref),
            ("q", wq_hbm, wq_ref),
            ("k", wk_hbm, wk_ref),
            ("v", wv_hbm, wv_ref),
            ("gate", gate_hbm, gate_ref),
            ("up", up_hbm, up_ref),
            ("down", down_hbm, down_ref),
            ("out", out_hbm, out_ref),
        )
    ):
        loads[name] = pltpu.make_async_copy(src, dst, load_sem.at[n])
        loads[name].start()

    nz = lax.axis_size("z")
    z, c = lax.axis_index("z"), lax.axis_index("c")
    y, x = lax.axis_index("y"), lax.axis_index("x")
    here = {"x": x, "y": y}
    part = y * 4 + x
    device = z * 2 + c
    half_z = nz // 2
    started = []

    def at_z(delta):
        return lax.rem(z + delta + nz, nz)

    barrier = pltpu.get_barrier_semaphore()
    peers = 0
    for dz in range(nz):
        for k in range(2):
            if dz or k:
                pl.semaphore_signal(
                    barrier,
                    inc=1,
                    device_id={"z": at_z(dz), "c": lax.rem(c + k, 2)},
                    device_id_type=MESH,
                )
                peers += 1
    for oy in range(4):
        for ox in range(4):
            if oy or ox:
                pl.semaphore_signal(
                    barrier,
                    inc=1,
                    device_id={"y": lax.rem(y + oy, 4), "x": lax.rem(x + ox, 4)},
                    device_id_type=MESH,
                )
                peers += 1

    top, tokens = routes_ref.shape
    experts = outgoing_ref.shape[0]
    table = columns_of(routes_ref[...], weight_ref[...])
    places = places_of(table, top, experts)
    first = (2 * part).astype(F32)
    select = selection_of(table, places, top, experts, first)
    loads["tokens"].wait()
    normed_b = rms_scale(tokens_ref[...], token_gain_ref[...])
    picked[...] = lax.dot_general(
        select, normed_b, (((0,), (0,)), ((), ())), preferred_element_type=F32
    ).astype(BF)
    for e in range(experts):
        outgoing_ref[e] = picked[2 * e : 2 * e + 2, :]

    pl.semaphore_wait(barrier, peers)

    def dispatch(o, k):
        zt, ct = at_z(SHIFT_Z - o), lax.rem(c + k, 2)
        return pltpu.make_async_remote_copy(
            src_ref=outgoing_ref.at[zt * 2 + ct],
            dst_ref=arrived.at[o * 2 + c],
            send_sem=sent_send.at[o * 2 + k],
            recv_sem=sent_recv.at[o * 2 + k],
            device_id={"z": zt, "c": ct},
            device_id_type=MESH,
        )

    order = sorted(range(nz), key=lambda o: (o >= half_z, -abs(SHIFT_Z - o)))
    for o in order:
        for k in range(2):
            if o == SHIFT_Z and k == 0:
                continue
            copy = dispatch(o, k)
            copy.start()
            started.append(copy)
    arrived[SHIFT_Z * 2 + c] = outgoing_ref[device]

    def pass_on(block, src, index, target):
        copy = pltpu.make_async_remote_copy(
            src_ref=src,
            dst_ref=kv.at[block],
            send_sem=kv_send.at[index],
            recv_sem=kv_recv.at[index],
            device_id=target,
            device_id_type=MESH,
        )
        copy.start()
        started.append(copy)

    def got(block, index):
        pltpu.make_async_remote_copy(
            src_ref=kv.at[block],
            dst_ref=kv.at[block],
            send_sem=kv_send.at[index],
            recv_sem=kv_recv.at[index],
            device_id={"c": 1 - c},
            device_id_type=MESH,
        ).wait_recv()

    ups, downs = half_z, half_z - 1
    up0, down0 = -1, ups - 1
    pup0, pdown0 = ups + downs, 2 * ups + downs

    def onward(distance, src, block, sign):
        base, most = (up0, ups) if sign > 0 else (down0, downs)
        for hop in (2, 1):
            if distance + hop <= most:
                pass_on(block, src, base + distance + hop, {"z": at_z(sign * hop)})

    def to_partner(distance, src, block, sign):
        base = pup0 if sign > 0 else pdown0
        pass_on(block, src, base + distance, {"c": 1 - c})

    def arrival(distance, sign):
        block = at_z(-sign * distance) * 2 + c
        got(block, (up0 if sign > 0 else down0) + distance)
        if distance % 2 == 0:
            onward(distance, kv.at[block], block, sign)
        to_partner(distance, kv.at[block], block, sign)

    def ring(step):
        if step == 0:
            onward(0, packed_ref, device, 1)
            onward(0, packed_ref, device, -1)
            to_partner(0, packed_ref, device, 1)
            kv[device] = packed_ref[...]
            return
        for distance in (2 * step, 2 * step - 1):
            arrival(distance, 1)
            if distance <= downs:
                arrival(distance, -1)

    def partner(distance, sign=1):
        got(at_z(-sign * distance) * 2 + 1 - c, (pup0 if sign > 0 else pdown0) + distance)

    length, head = query_ref.shape

    def stick(anchor, allowed=None):
        packed = kv[anchor]
        scores = lax.dot_general(
            query_ref[...],
            packed[:, :head],
            (((1,), (1,)), ((), ())),
            preferred_element_type=F32,
        )
        scores = scores + shift_ref[anchor]
        tail = jnp.log(1.0 + jnp.exp(-jnp.abs(scores)))
        soft = jnp.maximum(scores, 0.0) + tail
        if allowed is not None:
            soft = jnp.where(allowed, soft, 0.0)
        high = soft.astype(BF)
        low = (soft - high.astype(F32)).astype(BF)
        after = jnp.dot(high, triangle_ref[...], preferred_element_type=F32)
        after = after + jnp.dot(low, triangle_ref[...], preferred_element_type=F32)
        return jnp.minimum(scores, 0.0) - tail - after, after[:, :1] + soft[:, :1], packed[:, head:]

    def values_of(exponent, valued, allowed=None):
        weights = jnp.exp(exponent)
        if allowed is not None:
            weights = jnp.where(allowed, weights, 0.0)
        return jnp.dot(weights.astype(BF), valued, preferred_element_type=F32)

    def attend_diagonal():
        square = (length, length)
        triangle_ref[...] = (iota(square, 0) > iota(square, 1)).astype(F32).astype(BF)
        allowed = iota(square, 1) < iota(square, 0)
        exponent, total, valued = stick(device, allowed)
        running[...] = values_of(exponent, valued, allowed)
        carry[...] = total

    def attend_own():
        @pl.when(c == 1)
        def _():
            exponent, total, valued = stick(device - 1)
            running[...] += values_of(exponent - carry[...], valued)
            carry[...] += total

    def attend(first, last):
        def one(distance, none):
            near = (z - distance) * 2 + 1
            exponent, total, valued = stick(near)
            exponent2, total2, valued2 = stick(near - 1)
            before = carry[...]
            between = before + total
            running[...] += values_of(exponent - before, valued) + values_of(
                exponent2 - between, valued2
            )
            carry[...] = between + total2
            return none

        lax.fori_loop(first, jnp.minimum(last, z) + 1, one, 0)

    def gathering(number, piece):
        return Plane(piece, plane_recv.at[number], plane_send.at[number], here)

    gathers = [
        gathering(0, lambda slot, half: rows.at[0, slot * 2 + half]),
        gathering(1, lambda slot, half: rows.at[1, slot * 2 + half]),
        gathering(2, lambda slot, half: hidden.at[0, slot * 2 + half]),
        gathering(3, lambda slot, half: hidden.at[1, slot * 2 + half]),
    ]
    rows0, rows1, hidden0, hidden1 = gathers

    def lay_out(group):
        for o in range(group * half_z, (group + 1) * half_z):
            for k in range(2):
                if o == SHIFT_Z and k == 0:
                    continue
                zs, cs = at_z(o - SHIFT_Z), lax.rem(c + k, 2)
                pltpu.make_async_remote_copy(
                    src_ref=outgoing_ref.at[zs * 2 + cs],
                    dst_ref=arrived.at[o * 2 + cs],
                    send_sem=sent_send.at[o * 2 + k],
                    recv_sem=sent_recv.at[o * 2 + k],
                    device_id={"z": zs, "c": cs},
                    device_id_type=MESH,
                ).wait_recv()
        for n in range(nz):
            half, line = divmod(n, half_z)
            rows[group, part * 2 + half, 2 * line : 2 * line + 2, :] = arrived[group * nz + n]

    def expand(group):
        both = jnp.concatenate([gate_ref[...], up_ref[...]], axis=1)
        units = gate_ref.shape[1]

        def one(n, none):
            block = rows[group, pl.ds(n * 8, 8)].reshape(128, -1)
            flat = jnp.dot(block, both, preferred_element_type=F32)
            gating = jnp.minimum(flat[:, :units], glu_limit)
            linear = jnp.clip(flat[:, units:], -glu_limit, glu_limit)
            value = gating * jax.nn.sigmoid(glu_alpha * gating) * (linear + 1.0)
            where = pl.multiple_of(lax.rem(n, 2) * 128, 128)
            hidden[group, part * 2 + n // 2, pl.ds(where, 128), :] = value.astype(BF)
            return none

        lax.fori_loop(0, 4, one, 0)

    def contract(group):
        total = 512
        results = []
        for half in range(2):
            result = jnp.zeros((256, 128), F32)
            for pair in range(8):
                units = jnp.concatenate(
                    [hidden[group, 4 * pair + half], hidden[group, 4 * pair + 2 + half]], axis=1
                )
                result = result + jnp.dot(
                    units, down_ref[pair * 256 : (pair + 1) * 256], preferred_element_type=F32
                )
            results.append(result.astype(BF))
        stacked = jnp.concatenate(results, axis=0)
        to, of = iota((total, total), 0), iota((total, total), 1)
        source = ((to >> 1) & 15) * 32 + (to >> 5) * 2 + (to & 1)
        turned = jnp.dot(
            (source == of).astype(F32).astype(BF), stacked, preferred_element_type=F32
        ).astype(BF)
        leaving[group] = turned.reshape(nz, 32, 128)

    def send_back(o, k):
        zt, ct = at_z(o - SHIFT_Z), lax.rem(c + k, 2)
        group, line = divmod(o, half_z)
        return pltpu.make_async_remote_copy(
            src_ref=leaving.at[group, line * 2 + ct],
            dst_ref=returned.at[device],
            send_sem=back_send.at[o * 2 + k],
            recv_sem=back_recv.at[o * 2 + k],
            device_id={"z": zt, "c": ct},
            device_id_type=MESH,
        )

    def give_back(group):
        for o in order:
            if o // half_z != group:
                continue
            for k in range(2):
                if o == SHIFT_Z and k == 0:
                    continue
                copy = send_back(o, k)
                copy.start()
                started.append(copy)
        if group == 0:
            returned[device] = leaving[0, SHIFT_Z * 2 + c]

    def head_copy(oy, ox):
        index = ((-oy) % 4) * 4 + (-ox) % 4
        return pltpu.make_async_remote_copy(
            src_ref=heads.at[part],
            dst_ref=heads.at[part],
            send_sem=head_send.at[oy * 4 + ox],
            recv_sem=head_recv.at[index],
            device_id={"y": lax.rem(y + oy, 4), "x": lax.rem(x + ox, 4)},
            device_id_type=MESH,
        )

    def head_wait(oy, ox):
        slot = lax.rem(y + oy, 4) * 4 + lax.rem(x + ox, 4)
        pltpu.make_async_remote_copy(
            src_ref=heads.at[slot],
            dst_ref=heads.at[slot],
            send_sem=head_send.at[oy * 4 + ox],
            recv_sem=head_recv.at[oy * 4 + ox],
            device_id={"y": lax.rem(y + oy, 4), "x": lax.rem(x + ox, 4)},
            device_id_type=MESH,
        ).wait_recv()

    def project():
        for name in ("rows", "q", "k", "v"):
            loads[name].wait()
        normed = rms_scale(source_ref[...], gain_ref[...])

        def product(weight_ref):
            return lax.dot_general(
                normed, weight_ref[...], (((1,), (1,)), ((), ())), preferred_element_type=F32
            ).astype(BF)

        query_ref[...] = product(wq_ref) * BF(head ** (-0.5))
        packed_ref[:, :head] = product(wk_ref)
        packed_ref[:, head:] = product(wv_ref)

    def tables():
        for n, term in enumerate(combine_of(table, places, top, experts, 32)):
            combine_ref[n] = term

    def send_heads():
        for oy in range(4):
            for ox in range(4):
                if oy or ox:
                    copy = head_copy(oy, ox)
                    copy.start()
                    started.append(copy)

    def wait_heads():
        for oy in range(4):
            for ox in range(4):
                if oy or ox:
                    head_wait(oy, ox)

    def store_heads():
        summed = running[...].astype(BF)
        heads[part, :, :head] = summed[: length // 2]
        heads[part, :, head:] = summed[length // 2 :]

    project()
    ring(0)
    attend_diagonal()
    lay_out(0)
    rows0.stage0()
    tables()
    rows0.stage1()
    rows0.stage2()
    lay_out(1)
    rows1.stage0()
    rows0.stage3()
    ring(1)
    partner(0)
    attend_own()
    rows1.stage1()
    for name in ("gate", "up", "down", "out"):
        loads[name].wait()
    rows0.stage4()
    expand(0)
    ring(2)
    hidden0.stage0()
    rows1.stage2()
    partner(1)
    partner(2)
    attend(1, 2)
    rows1.stage3()
    ring(3)
    hidden0.stage1()
    rows1.stage4()
    expand(1)
    partner(3)
    partner(4)
    hidden1.stage0()
    attend(3, 4)
    hidden0.stage2()
    ring(4)
    hidden0.stage3()
    partner(5)
    partner(6)
    attend(5, 6)
    hidden1.stage1()
    partner(7)
    partner(8)
    attend(7, 8)
    hidden0.stage4()
    contract(0)
    for step in range(1, downs + 1):
        partner(step, -1)
    give_back(0)
    hidden1.stage2()
    attend(9, 11)
    hidden1.stage3()
    attend(12, nz - 1)
    store_heads()
    hidden1.stage4()
    send_heads()
    contract(1)
    give_back(1)
    wait_heads()
    mixed = jnp.zeros((length, 128), F32)
    for n in range(16):
        pair = heads[n]
        lines = jnp.concatenate([pair[:, :head], pair[:, head:]], axis=0)
        mixed = mixed + jnp.dot(
            lines, out_ref[n * head : (n + 1) * head], preferred_element_type=F32
        )
    mixer_ref[...] = mixed.astype(BF)

    for o in range(nz):
        for k in range(2):
            if o == SHIFT_Z and k == 0:
                continue
            zt, ct = at_z(SHIFT_Z - o), lax.rem(c + k, 2)
            pltpu.make_async_remote_copy(
                src_ref=returned.at[zt * 2 + ct],
                dst_ref=returned.at[zt * 2 + ct],
                send_sem=back_send.at[o * 2 + k],
                recv_sem=back_recv.at[o * 2 + k],
                device_id={"z": zt, "c": ct},
                device_id_type=MESH,
            ).wait_recv()
    results = returned[...].reshape(-1, 128)
    final = jnp.dot(combine_ref[0], results, preferred_element_type=F32)
    for n in range(1, 3):
        final = final + jnp.dot(combine_ref[n], results, preferred_element_type=F32)
    expert_ref[...] = final.astype(BF)

    for copy in started:
        copy.wait_send()
    for gather in gathers:
        gather.finish()


def per_device(
    mixer_rows,
    mixer_gain,
    w_query,
    w_key,
    w_value,
    key_shift,
    w_out,
    expert_rows,
    expert_gain,
    routes,
    route_weight,
    w_gate,
    w_up,
    w_down,
):
    length, width = mixer_rows.shape
    head = w_query.shape[1]
    tokens = expert_rows.shape[0]
    blocks = lax.axis_size("z") * 2
    cap = 2 * lax.axis_size("y") * lax.axis_size("x")
    vmem = pl.BlockSpec(memory_space=pltpu.VMEM)
    hbm = pl.BlockSpec(memory_space=pl.ANY)
    dma = pltpu.SemaphoreType.DMA
    v = pltpu.VMEM
    return pl.pallas_call(
        main_kernel,
        out_shape=(
            jax.ShapeDtypeStruct((length, 128), BF),
            jax.ShapeDtypeStruct((tokens, 128), BF),
        ),
        in_specs=[hbm, vmem, hbm, hbm, hbm, vmem, hbm, hbm, vmem, vmem, vmem, hbm, hbm, hbm],
        out_specs=(vmem,) * 2,
        scratch_shapes=[
            v((length, width), BF),
            v((head, width), BF),
            v((head, width), BF),
            v((head, width), BF),
            v(w_out.shape, BF),
            v((tokens, width), BF),
            v(w_gate.shape[1:], BF),
            v(w_up.shape[1:], BF),
            v(w_down.shape[1:], BF),
            v((length, head), BF),
            v((length, 2 * head), BF),
            v((blocks * 2, width), BF),
            v((blocks, 2, width), BF),
            v((3, tokens, blocks * cap), BF),
            v((length, length), BF),
            v((blocks, 2, width), BF),
            v((2, 32, 16, width), BF),
            v((2, 32, 256, 128), BF),
            v((2, blocks // 2, 32, 128), BF),
            v((blocks, 32, 128), BF),
            v((blocks, length, 2 * head), BF),
            v((16, length // 2, 2 * head), BF),
            v((length, head), F32),
            v((length, 1), F32),
            dma((9,)),
            dma((blocks,)),
            dma((blocks,)),
            dma((4, 2, 16)),
            dma((4, 2, 16)),
            dma((blocks,)),
            dma((blocks,)),
            dma((16,)),
            dma((16,)),
            dma((blocks,)),
            dma((blocks,)),
        ],
        compiler_params=pltpu.CompilerParams(
            collective_id=0, has_side_effects=True, vmem_limit_bytes=64000 * 1024
        ),
        name="main",
    )(
        mixer_rows,
        mixer_gain.reshape(1, -1),
        w_query.T,
        w_key.T,
        w_value.T,
        key_shift.reshape(-1, 1, length),
        w_out,
        expert_rows,
        expert_gain.reshape(1, -1),
        routes.T,
        route_weight.T,
        w_gate[0],
        w_up[0],
        w_down[0],
    )


def solution(mesh):
    torus = Mesh(mesh.devices.reshape(16, 2, 4, 4), ("z", "c", "y", "x"))
    return jax.shard_map(
        per_device,
        mesh=torus,
        in_specs=(
            P(EP, None),
            P(),
            P(None, TP),
            P(None, TP),
            P(None, TP),
            P(TP, None),
            P(None, TP),
            P(EP, None),
            P(),
            P(EP, None),
            P(EP, None),
            P(EP, None, TP),
            P(EP, None, TP),
            P(EP, None, TP),
        ),
        out_specs=(P(EP, TP), P(EP, TP)),
        check_vma=False,
    )
```

```python
import jax
import jax.numpy as jnp
from jax import lax
from jax.experimental import pallas as pl
from jax.experimental.pallas import tpu as pltpu
from jax.sharding import Mesh
from jax.sharding import PartitionSpec as P

MESH = pl.DeviceIdType.MESH
EP = ("z", "c")
TP = ("y", "x")
BF = jnp.bfloat16
F32 = jnp.float32

norm_eps = 1e-06
glu_limit = 7.0
glu_alpha = 1.702

SHIFT_Z = 3


def iota(shape, dim):
    return lax.broadcasted_iota(jnp.int32, shape, dim)


def rms_scale(source, scaling):
    floats = source.astype(F32)
    inverse = lax.rsqrt(jnp.mean(floats * floats, axis=-1, keepdims=True) + norm_eps)
    return (floats * inverse * scaling).astype(BF)


def split_three(value):
    high = value.astype(BF)
    rest = value - high.astype(F32)
    middle = rest.astype(BF)
    low = (rest - middle.astype(F32)).astype(BF)
    return high, middle, low


def columns_of(routes, weights):
    top, tokens = routes.shape
    fill = jnp.zeros((128 - 2 * top, tokens), F32)
    stacked = jnp.concatenate([routes.astype(F32), weights, fill], axis=0)
    return jnp.transpose(stacked)


def places_of(table, top, experts):
    tokens = table.shape[0]
    lanes = iota((tokens, experts), 1).astype(F32)
    hits = jnp.zeros((tokens, experts), F32)
    for k in range(top):
        hits = hits + (table[:, k : k + 1] == lanes).astype(F32)
    earlier = (iota((tokens, tokens), 1) < iota((tokens, tokens), 0)).astype(F32).astype(BF)
    counts = jnp.dot(earlier, hits.astype(BF), preferred_element_type=F32)
    return [
        jnp.sum(jnp.where(table[:, k : k + 1] == lanes, counts, 0.0), axis=1, keepdims=True)
        for k in range(top)
    ]


def selection_of(table, places, top, experts, parity, firsts):
    tokens = table.shape[0]
    slots = iota((tokens, experts * 2), 1).astype(F32)
    select = jnp.zeros((tokens, experts * 2), F32)
    for k in range(top):
        expert = table[:, k : k + 1]
        here = expert - 2.0 * jnp.floor(expert * 0.5) == parity
        for core, first in enumerate(firsts):
            own = places[k] - first
            line = (expert - parity + core) * 2.0 + own
            wanted = jnp.where(here & (own >= 0.0) & (own < 2.0), line, -1.0)
            select = select + (wanted == slots).astype(F32)
    return select.astype(BF)


def combine_of(table, places, top, experts, cap):
    tokens = table.shape[0]
    spots = iota((tokens, experts * cap), 1).astype(F32)
    combine = jnp.zeros((tokens, experts * cap), F32)
    for k in range(top):
        spot = table[:, k : k + 1] * float(cap) + places[k]
        combine = combine + jnp.where(spot == spots, table[:, top + k : top + k + 1], 0.0)
    return split_three(combine)


class Plane:
    def __init__(self, pieces, order, recv, send, here, up):
        self.pieces, self.order = pieces, order
        self.recv, self.send, self.here, self.up = recv, send, here, up
        self.sent = 0

    def piece(self, slot, part):
        return self.pieces.at[self.order(slot, part)]

    def bulk(self, number, recv=None):
        ref = self.pieces.at[pl.ds(0, number)]
        return pltpu.make_async_remote_copy(
            src_ref=ref,
            dst_ref=ref,
            send_sem=self.send,
            recv_sem=self.recv.at[0, 0] if recv is None else recv,
            device_id={"c": 1 - self.here["c"]},
            device_id_type=MESH,
        )

    def slot(self, f, s):
        column = self.here["l"]
        if f:
            column = column + 1 - 2 * lax.rem(column, 2)
        return lax.rem(self.here["y"] + s + 4, 4) * 4 + column

    def put(self, part, f, s, where):
        axis, delta = where
        h = self.here
        if axis == "x":
            target, index = {"x": h["x"] + 1 - 2 * lax.rem(h["x"], 2)}, (1 - f) * 4 + s % 4
        elif axis == "y":
            target, index = {"y": lax.rem(h["y"] + delta + 4, 4)}, f * 4 + (s - delta) % 4
        else:
            target, index = {"c": 1 - h["c"]}, 8
        ref = self.piece(self.slot(f, s), part)
        copy = pltpu.make_async_remote_copy(
            src_ref=ref,
            dst_ref=ref,
            send_sem=self.send,
            recv_sem=self.recv.at[part, index],
            device_id=target,
            device_id_type=MESH,
        )
        copy.start()
        self.sent += 1

    def take(self, part, f, s):
        ref = self.piece(self.slot(f, s), part)
        pltpu.make_async_remote_copy(
            src_ref=ref,
            dst_ref=ref,
            send_sem=self.send,
            recv_sem=self.recv.at[part, f * 4 + s % 4],
            device_id={"c": 1 - self.here["c"]},
            device_id_type=MESH,
        ).wait_recv()

    def along_y(self, part, f):
        for delta in (1, -1):
            self.put(part, f, 0, ("y", delta))

    def stage0a(self):
        self.put(0, 0, 0, ("x", 0))
        self.along_y(1, 0)

    def stage0b(self):
        self.along_y(0, 0)
        self.put(1, 0, 0, ("x", 0))
        for part in range(2):
            self.put(part, 0, 0, ("c", 0))

    def stage1(self):
        up = self.up
        self.take(1, 0, -up)
        self.put(1, 0, -up, ("y", up))
        self.put(1, 0, -up, ("x", 0))
        self.take(0, 1, 0)
        self.along_y(0, 1)
        self.take(1, 0, up)
        self.put(1, 0, up, ("x", 0))
        self.put(0, 1, 0, ("c", 0))
        self.put(1, 0, -up, ("c", 0))
        self.put(1, 0, up, ("c", 0))

    def stage2(self):
        for f, sign in ((0, -self.up), (1, self.up)):
            self.take(0, f, -sign)
            self.put(0, f, -sign, ("y", sign))
            self.put(0, f, -sign, ("c", 0))
            if f == 0:
                self.take(1, 0, 2)
                self.put(1, 0, 2, ("x", 0))
                self.put(1, 0, 2, ("c", 0))

    def stage3(self):
        for f, sign in ((0, -self.up), (1, self.up)):
            self.take(0, f, sign)
            self.put(0, f, sign, ("c", 0))
        for s in (0, -self.up, self.up, 2):
            self.take(1, 1, s)
            self.put(1, 1, s, ("c", 0))

    def stage4(self):
        for f in range(2):
            self.take(0, f, 2)
            self.put(0, f, 2, ("c", 0))
        for part in range(2):
            self.bulk(8, self.recv.at[part, 8]).wait_recv()

    def finish(self):
        self.bulk(self.sent).wait_send()


def main_kernel(
    rows_hbm,
    gain_ref,
    wq_hbm,
    wk_hbm,
    wv_hbm,
    shift_ref,
    out_hbm,
    tokens_hbm,
    token_gain_ref,
    routes_ref,
    weight_ref,
    gate_hbm,
    up_hbm,
    down_hbm,
    mixer_ref,
    expert_ref,
    source_ref,
    wq_ref,
    wk_ref,
    wv_ref,
    out_ref,
    tokens_ref,
    gate_ref,
    up_ref,
    down_ref,
    query_ref,
    packed_ref,
    picked,
    outgoing_ref,
    combine_ref,
    triangle_ref,
    arrived,
    rows,
    hidden,
    leaving,
    returned,
    kv,
    heads,
    running,
    carry,
    load_sem,
    trade_recv,
    trade_send,
    sent_recv,
    sent_send,
    plane_recv,
    plane_send,
    kv_recv,
    kv_send,
    head_recv,
    head_send,
    back_recv,
    back_send,
):
    loads = {}
    for n, (name, src, dst) in enumerate(
        (
            ("tokens", tokens_hbm, tokens_ref),
            ("rows", rows_hbm, source_ref),
            ("q", wq_hbm, wq_ref),
            ("k", wk_hbm, wk_ref),
            ("v", wv_hbm, wv_ref),
            ("gate", gate_hbm, gate_ref.at[0]),
            ("up", up_hbm, up_ref.at[0]),
            ("down", down_hbm, down_ref.at[0]),
            ("out", out_hbm, out_ref),
        )
    ):
        loads[name] = pltpu.make_async_copy(src, dst, load_sem.at[n])
        loads[name].start()

    nz = lax.axis_size("z")
    z, c = lax.axis_index("z"), lax.axis_index("c")
    y, x = lax.axis_index("y"), lax.axis_index("x")
    side = x // 2
    traded = lax.rem(side + c, 2)
    column = x + traded * (3 - 2 * x)
    here = {"x": x, "y": y, "c": c, "l": column}
    spot = y * 4 + column
    expert_here = z * 2 + side
    part = y * 4 + x
    device = z * 2 + c
    half_z = nz // 2

    def at_z(delta):
        return lax.rem(z + delta + nz, nz)

    barrier = pltpu.get_barrier_semaphore()
    peers = 0
    for dz in range(nz):
        for k in range(2):
            if dz or k:
                pl.semaphore_signal(
                    barrier,
                    inc=1,
                    device_id={"z": at_z(dz), "c": lax.rem(c + k, 2)},
                    device_id_type=MESH,
                )
                peers += 1
    for dz in range(nz):
        for k in range(2):
            pl.semaphore_signal(
                barrier,
                inc=1,
                device_id={"z": at_z(dz), "c": lax.rem(c + k, 2), "x": 3 - x},
                device_id_type=MESH,
            )
            peers += 1
    for oy in range(4):
        for ox in range(4):
            if oy or ox:
                pl.semaphore_signal(
                    barrier,
                    inc=1,
                    device_id={"y": lax.rem(y + oy, 4), "x": lax.rem(x + ox, 4)},
                    device_id_type=MESH,
                )
                peers += 1

    top, tokens = routes_ref.shape
    experts = outgoing_ref.shape[0]
    table = columns_of(routes_ref[...], weight_ref[...])
    places = places_of(table, top, experts)
    firsts = [
        (2 * (y * 4 + x + lax.rem(side + core, 2) * (3 - 2 * x))).astype(F32) for core in range(2)
    ]
    select = selection_of(table, places, top, experts, side.astype(F32), firsts)
    loads["tokens"].wait()
    normed_b = rms_scale(tokens_ref[...], token_gain_ref[...])
    picked[...] = lax.dot_general(
        select, normed_b, (((0,), (0,)), ((), ())), preferred_element_type=F32
    ).astype(BF)
    for e in range(experts):
        outgoing_ref[e] = picked[2 * e : 2 * e + 2, :]

    pl.semaphore_wait(barrier, peers)

    def dispatch(o, k):
        zt, ct = at_z(SHIFT_Z - o), lax.rem(c + k, 2)
        return pltpu.make_async_remote_copy(
            src_ref=outgoing_ref.at[zt * 2 + ct],
            dst_ref=arrived.at[o * 2 + c],
            send_sem=sent_send,
            recv_sem=sent_recv.at[o // half_z],
            device_id={"z": zt, "c": ct},
            device_id_type=MESH,
        )

    order = sorted(range(nz), key=lambda o: -min((o - SHIFT_Z) % nz, (SHIFT_Z - o) % nz))
    def send_out(group):
        for o in order:
            if o // half_z != group:
                continue
            for k in range(2):
                if o == SHIFT_Z and k == 0:
                    continue
                dispatch(o, k).start()
        if group == 0:
            arrived[SHIFT_Z * 2 + c] = outgoing_ref[device]

    def traded_copy(n):
        src, dst = ((gate_hbm, gate_ref), (up_hbm, up_ref), (down_hbm, down_ref))[n]
        return pltpu.make_async_remote_copy(
            src_ref=src,
            dst_ref=dst.at[1],
            send_sem=trade_send,
            recv_sem=trade_recv.at[n],
            device_id={"x": 3 - x, "c": 1 - c},
            device_id_type=MESH,
        )

    def trade():
        @pl.when(traded == 1)
        def _():
            for n in range(3):
                traded_copy(n).start()

    def traded_in(numbers):
        @pl.when(traded == 1)
        def _():
            for n in numbers:
                traded_copy(n).wait_recv()

    def pass_on(block, src, index, target):
        pltpu.make_async_remote_copy(
            src_ref=src,
            dst_ref=kv.at[block],
            send_sem=kv_send,
            recv_sem=kv_recv.at[index],
            device_id=target,
            device_id_type=MESH,
        ).start()

    def got(block, index):
        pltpu.make_async_remote_copy(
            src_ref=kv.at[block],
            dst_ref=kv.at[block],
            send_sem=kv_send,
            recv_sem=kv_recv.at[index],
            device_id={"c": 1 - c},
            device_id_type=MESH,
        ).wait_recv()

    ups, downs = half_z, half_z - 1
    up0, down0 = -1, ups - 1
    pup0, pdown0 = ups + downs, 2 * ups + downs

    def onward(distance, src, block, sign):
        base, most = (up0, ups) if sign > 0 else (down0, downs)
        for hop in (2, 1):
            if distance + hop <= most:
                pass_on(block, src, base + distance + hop, {"z": at_z(sign * hop)})

    def to_partner(distance, src, block, sign):
        base = pup0 if sign > 0 else pdown0
        pass_on(block, src, base + distance, {"c": 1 - c})

    def arrival(distance, sign):
        block = at_z(-sign * distance) * 2 + c
        got(block, (up0 if sign > 0 else down0) + distance)
        if distance % 2 == 0:
            onward(distance, kv.at[block], block, sign)
        to_partner(distance, kv.at[block], block, sign)

    def ring(step):
        if step == 0:
            onward(0, packed_ref, device, 1)
            onward(0, packed_ref, device, -1)
            to_partner(0, packed_ref, device, 1)
            return
        for distance in (2 * step, 2 * step - 1):
            arrival(distance, 1)
            if distance <= downs:
                arrival(distance, -1)

    def partner(distance, sign=1):
        got(at_z(-sign * distance) * 2 + 1 - c, (pup0 if sign > 0 else pdown0) + distance)

    length, head = query_ref.shape

    def stick(anchor, allowed=None):
        packed = kv[anchor]
        scores = lax.dot_general(
            query_ref[...],
            packed[:, :head],
            (((1,), (1,)), ((), ())),
            preferred_element_type=F32,
        )
        scores = scores + shift_ref[anchor]
        tail = jnp.log(1.0 + jnp.exp(-jnp.abs(scores)))
        soft = jnp.maximum(scores, 0.0) + tail
        if allowed is not None:
            soft = jnp.where(allowed, soft, 0.0)
        high = soft.astype(BF)
        low = (soft - high.astype(F32)).astype(BF)
        after = jnp.dot(high, triangle_ref[...], preferred_element_type=F32)
        after = after + jnp.dot(low, triangle_ref[...], preferred_element_type=F32)
        return jnp.minimum(scores, 0.0) - tail - after, after[:, :1] + soft[:, :1], packed[:, head:]

    def values_of(exponent, valued, allowed=None):
        weights = jnp.exp(exponent)
        if allowed is not None:
            weights = jnp.where(allowed, weights, 0.0)
        return jnp.dot(weights.astype(BF), valued, preferred_element_type=F32)

    def attend_diagonal():
        square = (length, length)
        triangle_ref[...] = (iota(square, 0) > iota(square, 1)).astype(F32).astype(BF)
        allowed = iota(square, 1) < iota(square, 0)
        exponent, total, valued = stick(device, allowed)
        running[...] = values_of(exponent, valued, allowed)
        carry[...] = total

    def attend_own():
        @pl.when(c == 1)
        def _():
            exponent, total, valued = stick(device - 1)
            running[...] += values_of(exponent - carry[...], valued)
            carry[...] += total

    def attend(first, last):
        def one(distance, none):
            near = (z - distance) * 2 + 1
            exponent, total, valued = stick(near)
            exponent2, total2, valued2 = stick(near - 1)
            before = carry[...]
            between = before + total
            running[...] += values_of(exponent - before, valued) + values_of(
                exponent2 - between, valued2
            )
            carry[...] = between + total2
            return none

        lax.fori_loop(first, jnp.minimum(last, z) + 1, one, 0)

    def gathering(number, pieces):
        sign = 1 if number in (0, 3) else -1

        def order(slot, part):
            return slot * 2 + part

        return Plane(pieces, order, plane_recv.at[number], plane_send.at[number], here, sign)

    gathers = [
        gathering(0, rows.at[0]),
        gathering(1, rows.at[1]),
        gathering(2, hidden.at[0]),
        gathering(3, hidden.at[1]),
    ]
    rows0, rows1, hidden0, hidden1 = gathers

    def lay_out(group):
        ref = arrived.at[pl.ds(0, nz - 1 + group)]
        pltpu.make_async_remote_copy(
            src_ref=ref,
            dst_ref=ref,
            send_sem=sent_send,
            recv_sem=sent_recv.at[group],
            device_id={"c": 1 - c},
            device_id_type=MESH,
        ).wait_recv()
        for n in range(nz):
            half, line = divmod(n, half_z)
            rows[group, spot * 2 + half, 2 * line : 2 * line + 2, :] = arrived[group * nz + n]

    def expand(group):
        both = jnp.concatenate([gate_ref[traded], up_ref[traded]], axis=1)
        units = gate_ref.shape[2]

        def one(n, none):
            block = rows[group, pl.ds(n * 8, 8)].reshape(128, -1)
            flat = jnp.dot(block, both, preferred_element_type=F32)
            gating = jnp.minimum(flat[:, :units], glu_limit)
            linear = jnp.clip(flat[:, units:], -glu_limit, glu_limit)
            value = gating * jax.nn.sigmoid(glu_alpha * gating) * (linear + 1.0)
            where = pl.multiple_of(lax.rem(n, 2) * 128, 128)
            hidden[group, spot * 2 + n // 2, pl.ds(where, 128), :] = value.astype(BF)
            return none

        lax.fori_loop(0, 4, one, 0)

    def contract(group):
        total = 512
        results = []
        for half in range(2):
            result = jnp.zeros((256, 128), F32)
            for pair in range(8):
                units = jnp.concatenate(
                    [hidden[group, 4 * pair + half], hidden[group, 4 * pair + 2 + half]], axis=1
                )
                result = result + jnp.dot(
                    units, down_ref[traded, pair * 256 : (pair + 1) * 256], preferred_element_type=F32
                )
            results.append(result.astype(BF))
        stacked = jnp.concatenate(results, axis=0)
        to, of = iota((total, total), 0), iota((total, total), 1)
        source = ((to >> 1) & 15) * 32 + (to >> 5) * 2 + (to & 1)
        turned = jnp.dot(
            (source == of).astype(F32).astype(BF), stacked, preferred_element_type=F32
        ).astype(BF)
        leaving[group] = turned.reshape(nz, 32, 128)

    def send_back(o, k):
        zt, ct = at_z(o - SHIFT_Z), lax.rem(c + k, 2)
        group, line = divmod(o, half_z)
        return pltpu.make_async_remote_copy(
            src_ref=leaving.at[group, line * 2 + ct],
            dst_ref=returned.at[expert_here],
            send_sem=back_send,
            recv_sem=back_recv,
            device_id={"z": zt, "c": ct, "x": column},
            device_id_type=MESH,
        )

    def give_back(group):
        for o in order:
            if o // half_z != group:
                continue
            for k in range(2):
                if o == SHIFT_Z and k == 0:

                    @pl.when(traded == 1)
                    def _():
                        send_back(SHIFT_Z, 0).start()

                    @pl.when(traded == 0)
                    def _():
                        returned[expert_here] = leaving[0, SHIFT_Z * 2 + c]

                    continue
                send_back(o, k).start()

    def bulk(ref, send, recv):
        return pltpu.make_async_remote_copy(
            src_ref=ref,
            dst_ref=ref,
            send_sem=send,
            recv_sem=recv,
            device_id={"c": 1 - c},
            device_id_type=MESH,
        )

    def of_all(wait):
        @pl.when(traded == 1)
        def _():
            wait(bulk(returned.at[pl.ds(0, 2 * nz)], back_send, back_recv))

        @pl.when(traded == 0)
        def _():
            wait(bulk(returned.at[pl.ds(0, 2 * nz - 1)], back_send, back_recv))

    def take_back():
        of_all(lambda copy: copy.wait_recv())

    def head_copy(oy, ox):
        return pltpu.make_async_remote_copy(
            src_ref=heads.at[part],
            dst_ref=heads.at[part],
            send_sem=head_send,
            recv_sem=head_recv,
            device_id={"y": lax.rem(y + oy, 4), "x": lax.rem(x + ox, 4)},
            device_id_type=MESH,
        )

    def project():
        for name in ("rows", "q", "k", "v"):
            loads[name].wait()
        normed = rms_scale(source_ref[...], gain_ref[...])

        def product(weight_ref):
            return lax.dot_general(
                normed, weight_ref[...], (((1,), (1,)), ((), ())), preferred_element_type=F32
            ).astype(BF)

        query_ref[...] = product(wq_ref) * BF(head ** (-0.5))
        packed_ref[:, :head] = product(wk_ref)
        packed_ref[:, head:] = product(wv_ref)
        kv[device] = packed_ref[...]

    def tables():
        for n, term in enumerate(combine_of(table, places, top, experts, 32)):
            combine_ref[n] = term

    def send_heads():
        for oy in range(4):
            for ox in range(4):
                if oy or ox:
                    head_copy(oy, ox).start()

    def wait_heads():
        bulk(heads.at[pl.ds(0, 15)], head_send, head_recv).wait_recv()

    def store_heads():
        summed = running[...].astype(BF)
        heads[part, :, :head] = summed[: length // 2]
        heads[part, :, head:] = summed[length // 2 :]

    def mix():
        mixed = jnp.zeros((length, 128), F32)
        for n in range(16):
            pair = heads[n]
            lines = jnp.concatenate([pair[:, :head], pair[:, head:]], axis=0)
            mixed = mixed + jnp.dot(
                lines, out_ref[n * head : (n + 1) * head], preferred_element_type=F32
            )
        mixer_ref[...] = mixed.astype(BF)

    def combine():
        results = returned[...].reshape(-1, 128)
        final = jnp.dot(combine_ref[0], results, preferred_element_type=F32)
        for n in range(1, 3):
            final = final + jnp.dot(combine_ref[n], results, preferred_element_type=F32)
        expert_ref[...] = final.astype(BF)

    def settle():
        bulk(arrived.at[pl.ds(0, 2 * nz - 1)], sent_send, sent_recv.at[0]).wait_send()
        bulk(kv.at[pl.ds(0, 2 * (ups + downs) + 1)], kv_send, kv_recv.at[0]).wait_send()
        bulk(heads.at[pl.ds(0, 15)], head_send, head_recv).wait_send()
        of_all(lambda copy: copy.wait_send())
        for gather in gathers:
            gather.finish()

        @pl.when(traded == 1)
        def _():
            bulk(gate_ref, trade_send, trade_recv.at[0]).wait_send()
            bulk(down_ref.at[0], trade_send, trade_recv.at[0]).wait_send()

    send_out(0)
    trade()
    project()
    send_out(1)
    attend_diagonal()
    lay_out(0)
    rows0.stage0a()
    rows0.stage0b()
    ring(0)
    tables()
    rows0.stage1()
    rows0.stage2()
    for name in ("gate", "up", "down", "out"):
        loads[name].wait()
    ring(1)
    lay_out(1)
    rows1.stage0a()
    rows1.stage0b()
    rows0.stage3()
    rows1.stage1()
    rows0.stage4()
    traded_in((0, 1))
    expand(0)
    hidden0.stage0a()
    ring(2)
    rows1.stage2()
    hidden0.stage0b()
    partner(0)
    attend_own()
    partner(1)
    partner(2)
    attend(1, 2)
    rows1.stage3()
    hidden0.stage1()
    rows1.stage4()
    expand(1)
    hidden1.stage0a()
    ring(3)
    partner(3)
    partner(4)
    attend(3, 4)
    hidden0.stage2()
    hidden1.stage0b()
    hidden0.stage3()
    hidden1.stage1()
    ring(4)
    partner(5)
    partner(6)
    attend(5, 6)
    hidden0.stage4()
    traded_in((2,))
    contract(0)
    give_back(0)
    partner(7)
    partner(8)
    attend(7, 8)
    hidden1.stage2()
    for step in range(1, downs + 1):
        partner(step, -1)
    attend(9, 11)
    hidden1.stage3()
    attend(12, nz - 1)
    store_heads()
    send_heads()
    hidden1.stage4()
    contract(1)
    give_back(1)
    wait_heads()
    mix()
    take_back()
    combine()
    settle()


def per_device(
    mixer_rows,
    mixer_gain,
    w_query,
    w_key,
    w_value,
    key_shift,
    w_out,
    expert_rows,
    expert_gain,
    routes,
    route_weight,
    w_gate,
    w_up,
    w_down,
):
    length, width = mixer_rows.shape
    head = w_query.shape[1]
    tokens = expert_rows.shape[0]
    blocks = lax.axis_size("z") * 2
    cap = 2 * lax.axis_size("y") * lax.axis_size("x")
    vmem = pl.BlockSpec(memory_space=pltpu.VMEM)
    hbm = pl.BlockSpec(memory_space=pl.ANY)
    dma = pltpu.SemaphoreType.DMA
    v = pltpu.VMEM
    return pl.pallas_call(
        main_kernel,
        out_shape=(
            jax.ShapeDtypeStruct((length, 128), BF),
            jax.ShapeDtypeStruct((tokens, 128), BF),
        ),
        in_specs=[hbm, vmem, hbm, hbm, hbm, vmem, hbm, hbm, vmem, vmem, vmem, hbm, hbm, hbm],
        out_specs=(vmem,) * 2,
        scratch_shapes=[
            v((length, width), BF),
            v((head, width), BF),
            v((head, width), BF),
            v((head, width), BF),
            v(w_out.shape, BF),
            v((tokens, width), BF),
            v((2, *w_gate.shape[1:]), BF),
            v((2, *w_up.shape[1:]), BF),
            v((2, *w_down.shape[1:]), BF),
            v((length, head), BF),
            v((length, 2 * head), BF),
            v((blocks * 2, width), BF),
            v((blocks, 2, width), BF),
            v((3, tokens, blocks * cap), BF),
            v((length, length), BF),
            v((blocks, 2, width), BF),
            v((2, 32, 16, width), BF),
            v((2, 32, 256, 128), BF),
            v((2, blocks // 2, 32, 128), BF),
            v((blocks, 32, 128), BF),
            v((blocks, length, 2 * head), BF),
            v((16, length // 2, 2 * head), BF),
            v((length, head), F32),
            v((length, 1), F32),
            dma((9,)),
            dma((3,)),
            dma,
            dma((2,)),
            dma,
            dma((4, 2, 9)),
            dma((4,)),
            dma((blocks - 1,)),
            dma,
            dma,
            dma,
            dma,
            dma,
        ],
        compiler_params=pltpu.CompilerParams(
            collective_id=0, has_side_effects=True, vmem_limit_bytes=64000 * 1024
        ),
        name="main",
    )(
        mixer_rows,
        mixer_gain.reshape(1, -1),
        w_query.T,
        w_key.T,
        w_value.T,
        key_shift.reshape(-1, 1, length),
        w_out,
        expert_rows,
        expert_gain.reshape(1, -1),
        routes.T,
        route_weight.T,
        w_gate[0],
        w_up[0],
        w_down[0],
    )


def solution(mesh):
    torus = Mesh(mesh.devices.reshape(16, 2, 4, 4), ("z", "c", "y", "x"))
    return jax.shard_map(
        per_device,
        mesh=torus,
        in_specs=(
            P(EP, None),
            P(),
            P(None, TP),
            P(None, TP),
            P(None, TP),
            P(TP, None),
            P(None, TP),
            P(EP, None),
            P(),
            P(EP, None),
            P(EP, None),
            P(EP, None, TP),
            P(EP, None, TP),
            P(EP, None, TP),
        ),
        out_specs=(P(EP, TP), P(EP, TP)),
        check_vma=False,
    )
```

```python
import jax
import jax.numpy as jnp
from jax import lax
from jax.experimental import pallas as pl
from jax.experimental.pallas import tpu as pltpu
from jax.sharding import Mesh
from jax.sharding import PartitionSpec as P

MESH = pl.DeviceIdType.MESH
EP = ("z", "c")
TP = ("y", "x")
BF = jnp.bfloat16
F32 = jnp.float32

norm_eps = 1e-06
glu_limit = 7.0
glu_alpha = 1.702

OFFSETS = (-1, 0, 1, 2, 8, 7, -7, -6, 6, 5, -5, -4, 4, 3, -3, -2)
GROUPS = 4
OWN = OFFSETS.index(0)


def iota(shape, dim):
    return lax.broadcasted_iota(jnp.int32, shape, dim)


def rms_scale(source, scaling):
    floats = source.astype(F32)
    inverse = lax.rsqrt(jnp.mean(floats * floats, axis=-1, keepdims=True) + norm_eps)
    return (floats * inverse * scaling).astype(BF)


def split_three(value):
    high = value.astype(BF)
    rest = value - high.astype(F32)
    middle = rest.astype(BF)
    low = (rest - middle.astype(F32)).astype(BF)
    return high, middle, low


def columns_of(routes, weights):
    top, tokens = routes.shape
    fill = jnp.zeros((128 - 2 * top, tokens), F32)
    stacked = jnp.concatenate([routes.astype(F32), weights, fill], axis=0)
    return jnp.transpose(stacked)


def places_of(table, top, experts):
    tokens = table.shape[0]
    lanes = iota((tokens, experts), 1).astype(F32)
    hits = jnp.zeros((tokens, experts), F32)
    for k in range(top):
        hits = hits + (table[:, k : k + 1] == lanes).astype(F32)
    earlier = (iota((tokens, tokens), 1) < iota((tokens, tokens), 0)).astype(F32).astype(BF)
    counts = jnp.dot(earlier, hits.astype(BF), preferred_element_type=F32)
    return [
        jnp.sum(jnp.where(table[:, k : k + 1] == lanes, counts, 0.0), axis=1, keepdims=True)
        for k in range(top)
    ]


def selection_of(table, places, top, experts, parity, firsts):
    tokens = table.shape[0]
    slots = iota((tokens, experts * 2), 1).astype(F32)
    select = jnp.zeros((tokens, experts * 2), F32)
    for k in range(top):
        expert = table[:, k : k + 1]
        here = expert - 2.0 * jnp.floor(expert * 0.5) == parity
        for core, first in enumerate(firsts):
            own = places[k] - first
            line = (expert - parity + core) * 2.0 + own
            wanted = jnp.where(here & (own >= 0.0) & (own < 2.0), line, -1.0)
            select = select + (wanted == slots).astype(F32)
    return select.astype(BF)


def combine_of(table, places, top, experts, cap):
    tokens = table.shape[0]
    spots = iota((tokens, experts * cap), 1).astype(F32)
    combine = jnp.zeros((tokens, experts * cap), F32)
    for k in range(top):
        spot = table[:, k : k + 1] * float(cap) + places[k]
        combine = combine + jnp.where(spot == spots, table[:, top + k : top + k + 1], 0.0)
    return split_three(combine)


class Plane:
    def __init__(self, pieces, order, recv, send, here, up):
        self.pieces, self.order = pieces, order
        self.recv, self.send, self.here, self.up = recv, send, here, up
        self.sent = 0

    def piece(self, slot, part):
        return self.pieces.at[self.order(slot, part)]

    def bulk(self, number, recv=None):
        ref = self.pieces.at[pl.ds(0, number)]
        return pltpu.make_async_remote_copy(
            src_ref=ref,
            dst_ref=ref,
            send_sem=self.send,
            recv_sem=self.recv.at[0, 0] if recv is None else recv,
            device_id={"c": 1 - self.here["c"]},
            device_id_type=MESH,
        )

    def slot(self, f, s):
        column = self.here["l"]
        if f:
            column = column + 1 - 2 * lax.rem(column, 2)
        return lax.rem(self.here["y"] + s + 4, 4) * 4 + column

    def put(self, part, f, s, where):
        axis, delta = where
        h = self.here
        if axis == "x":
            target, index = {"x": h["x"] + 1 - 2 * lax.rem(h["x"], 2)}, (1 - f) * 4 + s % 4
        elif axis == "y":
            target, index = {"y": lax.rem(h["y"] + delta + 4, 4)}, f * 4 + (s - delta) % 4
        else:
            target, index = {"c": 1 - h["c"]}, 8
        ref = self.piece(self.slot(f, s), part)
        copy = pltpu.make_async_remote_copy(
            src_ref=ref,
            dst_ref=ref,
            send_sem=self.send,
            recv_sem=self.recv.at[part, index],
            device_id=target,
            device_id_type=MESH,
        )
        copy.start()
        self.sent += 1

    def take(self, part, f, s):
        ref = self.piece(self.slot(f, s), part)
        pltpu.make_async_remote_copy(
            src_ref=ref,
            dst_ref=ref,
            send_sem=self.send,
            recv_sem=self.recv.at[part, f * 4 + s % 4],
            device_id={"c": 1 - self.here["c"]},
            device_id_type=MESH,
        ).wait_recv()

    def along_y(self, part, f):
        for delta in (1, -1):
            self.put(part, f, 0, ("y", delta))

    def stage0a(self):
        self.put(0, 0, 0, ("x", 0))
        self.along_y(1, 0)

    def stage0b(self):
        self.along_y(0, 0)
        self.put(1, 0, 0, ("x", 0))
        for part in range(2):
            self.put(part, 0, 0, ("c", 0))

    def stage1(self):
        up = self.up
        self.take(1, 0, -up)
        self.put(1, 0, -up, ("y", up))
        self.put(1, 0, -up, ("x", 0))
        self.take(0, 1, 0)
        self.along_y(0, 1)
        self.take(1, 0, up)
        self.put(1, 0, up, ("x", 0))
        self.put(0, 1, 0, ("c", 0))
        self.put(1, 0, -up, ("c", 0))
        self.put(1, 0, up, ("c", 0))

    def stage2(self):
        for f, sign in ((0, -self.up), (1, self.up)):
            self.take(0, f, -sign)
            self.put(0, f, -sign, ("y", sign))
            self.put(0, f, -sign, ("c", 0))
            if f == 0:
                self.take(1, 0, 2)
                self.put(1, 0, 2, ("x", 0))
                self.put(1, 0, 2, ("c", 0))

    def stage3(self):
        for f, sign in ((0, -self.up), (1, self.up)):
            self.take(0, f, sign)
            self.put(0, f, sign, ("c", 0))
        for s in (0, -self.up, self.up, 2):
            self.take(1, 1, s)
            self.put(1, 1, s, ("c", 0))

    def stage4(self):
        for f in range(2):
            self.take(0, f, 2)
            self.put(0, f, 2, ("c", 0))

    def stage5(self):
        for part in range(2):
            self.bulk(8, self.recv.at[part, 8]).wait_recv()

    def finish(self):
        self.bulk(self.sent).wait_send()


def main_kernel(
    rows_hbm,
    gain_ref,
    wq_hbm,
    wk_hbm,
    wv_hbm,
    shift_ref,
    out_hbm,
    tokens_hbm,
    token_gain_ref,
    routes_ref,
    weight_ref,
    gate_hbm,
    up_hbm,
    down_hbm,
    mixer_ref,
    expert_ref,
    source_ref,
    wq_ref,
    wk_ref,
    wv_ref,
    out_ref,
    tokens_ref,
    gate_ref,
    up_ref,
    down_ref,
    query_ref,
    packed_ref,
    picked,
    outgoing_ref,
    combine_ref,
    triangle_ref,
    arrived,
    rows,
    hidden,
    leaving,
    returned,
    kv,
    heads,
    running,
    carry,
    load_sem,
    trade_recv,
    trade_send,
    sent_recv,
    sent_send,
    plane_recv,
    plane_send,
    kv_recv,
    kv_send,
    head_recv,
    head_send,
    back_recv,
    back_send,
):
    loads = {}
    for n, (name, src, dst) in enumerate(
        (
            ("tokens", tokens_hbm, tokens_ref),
            ("rows", rows_hbm, source_ref),
            ("q", wq_hbm, wq_ref),
            ("k", wk_hbm, wk_ref),
            ("v", wv_hbm, wv_ref),
            ("gate", gate_hbm, gate_ref.at[0]),
            ("up", up_hbm, up_ref.at[0]),
            ("down", down_hbm, down_ref.at[0]),
            ("out", out_hbm, out_ref),
        )
    ):
        loads[name] = pltpu.make_async_copy(src, dst, load_sem.at[n])
        loads[name].start()

    nz = lax.axis_size("z")
    z, c = lax.axis_index("z"), lax.axis_index("c")
    y, x = lax.axis_index("y"), lax.axis_index("x")
    side = x // 2
    traded = lax.rem(side + c, 2)
    column = x + traded * (3 - 2 * x)
    here = {"x": x, "y": y, "c": c, "l": column}
    spot = y * 4 + column
    expert_here = z * 2 + side
    part = y * 4 + x
    device = z * 2 + c
    half_z = nz // 2
    chips = nz // GROUPS

    def at_z(delta):
        return lax.rem(z + delta + nz, nz)

    barrier = pltpu.get_barrier_semaphore()
    peers = 0
    for dz in range(nz):
        for k in range(2):
            if dz or k:
                pl.semaphore_signal(
                    barrier,
                    inc=1,
                    device_id={"z": at_z(dz), "c": lax.rem(c + k, 2)},
                    device_id_type=MESH,
                )
                peers += 1
    for dz in range(nz):
        for k in range(2):
            pl.semaphore_signal(
                barrier,
                inc=1,
                device_id={"z": at_z(dz), "c": lax.rem(c + k, 2), "x": 3 - x},
                device_id_type=MESH,
            )
            peers += 1
    for oy in range(4):
        for ox in range(4):
            if oy or ox:
                pl.semaphore_signal(
                    barrier,
                    inc=1,
                    device_id={"y": lax.rem(y + oy, 4), "x": lax.rem(x + ox, 4)},
                    device_id_type=MESH,
                )
                peers += 1

    top, tokens = routes_ref.shape
    experts = outgoing_ref.shape[0]
    table = columns_of(routes_ref[...], weight_ref[...])
    places = places_of(table, top, experts)
    firsts = [
        (2 * (y * 4 + x + lax.rem(side + core, 2) * (3 - 2 * x))).astype(F32) for core in range(2)
    ]
    select = selection_of(table, places, top, experts, side.astype(F32), firsts)
    loads["tokens"].wait()
    normed_b = rms_scale(tokens_ref[...], token_gain_ref[...])
    picked[...] = lax.dot_general(
        select, normed_b, (((0,), (0,)), ((), ())), preferred_element_type=F32
    ).astype(BF)
    for e in range(experts):
        outgoing_ref[e] = picked[2 * e : 2 * e + 2, :]

    pl.semaphore_wait(barrier, peers)

    def dispatch(o, k):
        zt, ct = at_z(-OFFSETS[o]), lax.rem(c + k, 2)
        return pltpu.make_async_remote_copy(
            src_ref=outgoing_ref.at[zt * 2 + ct],
            dst_ref=arrived.at[o * 2 + c],
            send_sem=sent_send,
            recv_sem=sent_recv.at[o // chips],
            device_id={"z": zt, "c": ct},
            device_id_type=MESH,
        )

    def order_of(group):
        return sorted(range(group * chips, (group + 1) * chips), key=lambda o: -abs(OFFSETS[o]))

    def send_out(group):
        for o in order_of(group):
            for k in range(2):
                if o == OWN and k == 0:
                    continue
                dispatch(o, k).start()
        if group == 0:
            arrived[OWN * 2 + c] = outgoing_ref[device]

    def traded_copy(n):
        src, dst = ((gate_hbm, gate_ref), (up_hbm, up_ref), (down_hbm, down_ref))[n]
        return pltpu.make_async_remote_copy(
            src_ref=src,
            dst_ref=dst.at[1],
            send_sem=trade_send,
            recv_sem=trade_recv.at[n],
            device_id={"x": 3 - x, "c": 1 - c},
            device_id_type=MESH,
        )

    def trade():
        @pl.when(traded == 1)
        def _():
            for n in range(3):
                traded_copy(n).start()

    def traded_in(numbers):
        @pl.when(traded == 1)
        def _():
            for n in numbers:
                traded_copy(n).wait_recv()

    def pass_on(block, src, index, target):
        pltpu.make_async_remote_copy(
            src_ref=src,
            dst_ref=kv.at[block],
            send_sem=kv_send,
            recv_sem=kv_recv.at[index],
            device_id=target,
            device_id_type=MESH,
        ).start()

    def got(block, index):
        pltpu.make_async_remote_copy(
            src_ref=kv.at[block],
            dst_ref=kv.at[block],
            send_sem=kv_send,
            recv_sem=kv_recv.at[index],
            device_id={"c": 1 - c},
            device_id_type=MESH,
        ).wait_recv()

    ups, downs = half_z, half_z - 1
    up0, down0 = -1, ups - 1
    pup0, pdown0 = ups + downs, 2 * ups + downs

    def onward(distance, src, block, sign):
        base, most = (up0, ups) if sign > 0 else (down0, downs)
        for hop in (2, 1):
            if distance + hop <= most:
                pass_on(block, src, base + distance + hop, {"z": at_z(sign * hop)})

    def to_partner(distance, src, block, sign):
        base = pup0 if sign > 0 else pdown0
        pass_on(block, src, base + distance, {"c": 1 - c})

    def arrival(distance, sign):
        block = at_z(-sign * distance) * 2 + c
        got(block, (up0 if sign > 0 else down0) + distance)
        if distance % 2 == 0:
            onward(distance, kv.at[block], block, sign)
        to_partner(distance, kv.at[block], block, sign)

    def ring(step):
        if step == 0:
            onward(0, packed_ref, device, 1)
            onward(0, packed_ref, device, -1)
            to_partner(0, packed_ref, device, 1)
            return
        for distance in (2 * step, 2 * step - 1):
            arrival(distance, 1)
            if distance <= downs:
                arrival(distance, -1)

    def partner(distance, sign=1):
        got(at_z(-sign * distance) * 2 + 1 - c, (pup0 if sign > 0 else pdown0) + distance)

    length, head = query_ref.shape

    def stick(anchor, allowed=None):
        packed = kv[anchor]
        scores = lax.dot_general(
            query_ref[...],
            packed[:, :head],
            (((1,), (1,)), ((), ())),
            preferred_element_type=F32,
        )
        scores = scores + shift_ref[anchor]
        tail = jnp.log(1.0 + jnp.exp(-jnp.abs(scores)))
        soft = jnp.maximum(scores, 0.0) + tail
        if allowed is not None:
            soft = jnp.where(allowed, soft, 0.0)
        after = jnp.dot(soft.astype(BF), triangle_ref[...], preferred_element_type=F32)
        return jnp.minimum(scores, 0.0) - tail - after, after[:, :1] + soft[:, :1], packed[:, head:]

    def values_of(exponent, valued, allowed=None):
        weights = jnp.exp(exponent)
        if allowed is not None:
            weights = jnp.where(allowed, weights, 0.0)
        return jnp.dot(weights.astype(BF), valued, preferred_element_type=F32)

    def attend_diagonal():
        square = (length, length)
        triangle_ref[...] = (iota(square, 0) > iota(square, 1)).astype(F32).astype(BF)
        allowed = iota(square, 1) < iota(square, 0)
        exponent, total, valued = stick(device, allowed)
        running[...] = values_of(exponent, valued, allowed)
        carry[...] = total

    def attend_own():
        @pl.when(c == 1)
        def _():
            exponent, total, valued = stick(device - 1)
            running[...] += values_of(exponent - carry[...], valued)
            carry[...] += total

    def attend(first, last):
        def one(distance, none):
            near = (z - distance) * 2 + 1
            exponent, total, valued = stick(near)
            exponent2, total2, valued2 = stick(near - 1)
            before = carry[...]
            between = before + total
            running[...] += values_of(exponent - before, valued) + values_of(
                exponent2 - between, valued2
            )
            carry[...] = between + total2
            return none

        lax.fori_loop(first, jnp.minimum(last, z) + 1, one, 0)

    def gathering(number, pieces):
        sign = 1 if number % 2 == 0 else -1

        def order(slot, part):
            return part * 16 + slot

        return Plane(pieces, order, plane_recv.at[number], plane_send.at[number], here, sign)

    rows_of = [gathering(n, rows.at[n]) for n in range(GROUPS)]
    hidden_of = [gathering(GROUPS + n, hidden.at[n]) for n in range(GROUPS)]
    gathers = rows_of + hidden_of
    half_width = rows.shape[3]

    def lay_out(group):
        lines = 2 * chips
        ref = arrived.at[pl.ds(0, lines - (group == 0))]
        pltpu.make_async_remote_copy(
            src_ref=ref,
            dst_ref=ref,
            send_sem=sent_send,
            recv_sem=sent_recv.at[group],
            device_id={"c": 1 - c},
            device_id_type=MESH,
        ).wait_recv()
        for line in range(lines):
            for half in range(2):
                rows[group, half * 16 + spot, 2 * line : 2 * line + 2, :] = arrived[
                    group * lines + line, :, half * half_width : (half + 1) * half_width
                ]

    def expand(group):
        both = jnp.concatenate([gate_ref[traded], up_ref[traded]], axis=1)
        units = gate_ref.shape[2]

        def one(n, none):
            first, second = (
                rows[group, pl.ds(half * 16 + n * 8, 8)].reshape(128, half_width)
                for half in range(2)
            )
            flat = jnp.dot(first, both[:half_width], preferred_element_type=F32)
            flat = flat + jnp.dot(second, both[half_width:], preferred_element_type=F32)
            gating = jnp.minimum(flat[:, :units], glu_limit)
            linear = jnp.clip(flat[:, units:], -glu_limit, glu_limit)
            value = gating * jax.nn.sigmoid(glu_alpha * gating) * (linear + 1.0)
            hidden[group, n * 16 + spot] = value.astype(BF)
            return none

        lax.fori_loop(0, 2, one, 0)

    def contract(group):
        total = 256
        result = jnp.zeros((total, 128), F32)
        for pair in range(8):
            units = jnp.concatenate(
                [
                    jnp.concatenate([hidden[group, n], hidden[group, 16 + n]], axis=0)
                    for n in (2 * pair, 2 * pair + 1)
                ],
                axis=1,
            )
            result = result + jnp.dot(
                units,
                down_ref[traded, pair * 256 : (pair + 1) * 256],
                preferred_element_type=F32,
            )
        to, of = iota((total, total), 0), iota((total, total), 1)
        source = ((to >> 1) & 15) * 16 + (to >> 5) * 2 + (to & 1)
        turned = jnp.dot(
            (source == of).astype(F32).astype(BF), result.astype(BF), preferred_element_type=F32
        ).astype(BF)
        leaving[group] = turned.reshape(2 * chips, 32, 128)

    def send_back(o, k):
        zt, ct = at_z(OFFSETS[o]), lax.rem(c + k, 2)
        group, line = divmod(o, chips)
        return pltpu.make_async_remote_copy(
            src_ref=leaving.at[group, line * 2 + ct],
            dst_ref=returned.at[expert_here],
            send_sem=back_send,
            recv_sem=back_recv,
            device_id={"z": zt, "c": ct, "x": column},
            device_id_type=MESH,
        )

    def give_back(group):
        for o in order_of(group):
            for k in range(2):
                if o == OWN and k == 0:

                    @pl.when(traded == 1)
                    def _():
                        send_back(OWN, 0).start()

                    @pl.when(traded == 0)
                    def _():
                        returned[expert_here] = leaving[0, OWN * 2 + c]

                    continue
                send_back(o, k).start()

    def bulk(ref, send, recv):
        return pltpu.make_async_remote_copy(
            src_ref=ref,
            dst_ref=ref,
            send_sem=send,
            recv_sem=recv,
            device_id={"c": 1 - c},
            device_id_type=MESH,
        )

    def of_all(wait):
        @pl.when(traded == 1)
        def _():
            wait(bulk(returned.at[pl.ds(0, 2 * nz)], back_send, back_recv))

        @pl.when(traded == 0)
        def _():
            wait(bulk(returned.at[pl.ds(0, 2 * nz - 1)], back_send, back_recv))

    def take_back():
        of_all(lambda copy: copy.wait_recv())

    def head_copy(oy, ox):
        return pltpu.make_async_remote_copy(
            src_ref=heads.at[part],
            dst_ref=heads.at[part],
            send_sem=head_send,
            recv_sem=head_recv,
            device_id={"y": lax.rem(y + oy, 4), "x": lax.rem(x + ox, 4)},
            device_id_type=MESH,
        )

    def project():
        for name in ("rows", "q", "k", "v"):
            loads[name].wait()
        normed = rms_scale(source_ref[...], gain_ref[...])

        def product(weight_ref):
            return lax.dot_general(
                normed, weight_ref[...], (((1,), (1,)), ((), ())), preferred_element_type=F32
            ).astype(BF)

        query_ref[...] = product(wq_ref) * BF(head ** (-0.5))
        packed_ref[:, :head] = product(wk_ref)
        packed_ref[:, head:] = product(wv_ref)
        kv[device] = packed_ref[...]

    def tables():
        for n, term in enumerate(combine_of(table, places, top, experts, 32)):
            combine_ref[n] = term

    def send_heads():
        for oy in range(4):
            for ox in range(4):
                if oy or ox:
                    head_copy(oy, ox).start()

    def wait_heads():
        bulk(heads.at[pl.ds(0, 15)], head_send, head_recv).wait_recv()

    def store_heads():
        summed = running[...].astype(BF)
        heads[part, :, :head] = summed[: length // 2]
        heads[part, :, head:] = summed[length // 2 :]

    def mix():
        mixed = jnp.zeros((length, 128), F32)
        for n in range(16):
            pair = heads[n]
            lines = jnp.concatenate([pair[:, :head], pair[:, head:]], axis=0)
            mixed = mixed + jnp.dot(
                lines, out_ref[n * head : (n + 1) * head], preferred_element_type=F32
            )
        mixer_ref[...] = mixed.astype(BF)

    def combine():
        results = returned[...].reshape(-1, 128)
        final = jnp.dot(combine_ref[0], results, preferred_element_type=F32)
        for n in range(1, 3):
            final = final + jnp.dot(combine_ref[n], results, preferred_element_type=F32)
        expert_ref[...] = final.astype(BF)

    def settle():
        bulk(arrived.at[pl.ds(0, 2 * nz - 1)], sent_send, sent_recv.at[0]).wait_send()
        bulk(kv.at[pl.ds(0, 2 * (ups + downs) + 1)], kv_send, kv_recv.at[0]).wait_send()
        bulk(heads.at[pl.ds(0, 15)], head_send, head_recv).wait_send()
        of_all(lambda copy: copy.wait_send())
        for gather in gathers:
            gather.finish()

        @pl.when(traded == 1)
        def _():
            bulk(gate_ref, trade_send, trade_recv.at[0]).wait_send()
            bulk(down_ref.at[0], trade_send, trade_recv.at[0]).wait_send()

    plan = []

    def due(time, name, work, *arguments):
        plan.append((time, len(plan), name, work, arguments))

    def load_weights():
        for name in ("gate", "up", "down", "out"):
            loads[name].wait()

    def expand_and_go(group):
        expand(group)
        hidden_of[group].stage0a()

    def contract_and_go(group):
        contract(group)
        give_back(group)

    def lay_out_and_go(group):
        lay_out(group)
        rows_of[group].stage0a()
        rows_of[group].stage0b()

    def partners(distances, sign=1):
        for distance in distances:
            partner(distance, sign)

    def pass_heads():
        store_heads()
        send_heads()

    def pass_heads_if(finished):
        pl.when(finished)(pass_heads)

    def attend_if(wanted, first, last):
        pl.when(wanted)(lambda: attend(first, last))

    due(0.0, "send", send_out, 0)
    due(0.1, "trade", trade)
    due(0.2, "send", send_out, 1)
    due(0.3, "project", project)
    due(0.4, "send", send_out, 2)
    due(4.0, "send", send_out, 3)
    due(0.6, "diagonal", attend_diagonal)
    due(3.0, "tables", tables)
    due(1.0, "ring", ring, 0)
    due(9.0, "weights", load_weights)
    for group, time in enumerate((5.5, 13.4, 15.0, 19.2)):
        due(time, f"lay{group}", lay_out_and_go, group)
        for kind, gather in (("rows", rows_of[group]), ("hidden", hidden_of[group])):
            tag = f"{kind}{group}"
            due(time + 3.4, tag + "_1", gather.stage1)
            due(time + 6.4, tag + "_2", gather.stage2)
            due(time + 9.2, tag + "_3", gather.stage3)
            due(time + 9.4, tag + "_4", gather.stage4)
            due(time + 11.0, tag + "_5", gather.stage5)
            time = time + 11.8
            if kind == "rows":
                if group == 0:
                    due(time - 0.5, "traded", traded_in, (0, 1))
                due(time - 0.4, f"expand{group}", expand_and_go, group)
                due(time - 0.2, f"hidden{group}_0", hidden_of[group].stage0b)
        if group == 0:
            due(time - 0.5, "traded", traded_in, (2,))
        due(time - 0.4, f"contract{group}", contract_and_go, group)
    due(16.7, "ring", ring, 1)
    due(18.6, "partners", partners, (0, 1, 2))
    due(18.7, "attend", attend_own)
    due(18.8, "attend", attend, 1, 2)
    due(21.6, "ring", ring, 2)
    due(23.8, "partners", partners, (3, 4))
    due(23.9, "attend", attend, 3, 4)
    due(26.6, "ring", ring, 3)
    due(28.75, "partners", partners, (5, 6))
    due(28.76, "attend", attend, 5, 6)
    due(34.45, "ring", ring, 4)
    due(38.3, "partners", partners, (7, 8))
    due(38.31, "attend", attend, 7, 8)
    due(38.32, "partners", partners, tuple(range(1, downs + 1)), -1)
    due(38.33, "attend", attend_if, z <= 10, 9, 10)
    due(42.55, "attend", attend_if, z > 10, 9, 10)
    due(42.6, "attend", attend, 11, 12)
    due(42.61, "attend", attend, 13, nz - 1)
    due(38.34, "heads", pass_heads_if, z <= 10)
    due(42.62, "heads", pass_heads_if, z > 10)
    due(80.0, "wait_heads", wait_heads)
    due(80.1, "mix", mix)
    due(80.2, "take_back", take_back)
    due(80.3, "combine", combine)
    due(80.4, "settle", settle)
    for _, _, name, work, arguments in sorted(plan, key=lambda entry: entry[:2]):
        with jax.named_scope(name):
            work(*arguments)


def per_device(
    mixer_rows,
    mixer_gain,
    w_query,
    w_key,
    w_value,
    key_shift,
    w_out,
    expert_rows,
    expert_gain,
    routes,
    route_weight,
    w_gate,
    w_up,
    w_down,
):
    length, width = mixer_rows.shape
    head = w_query.shape[1]
    tokens = expert_rows.shape[0]
    blocks = lax.axis_size("z") * 2
    cap = 2 * lax.axis_size("y") * lax.axis_size("x")
    vmem = pl.BlockSpec(memory_space=pltpu.VMEM)
    hbm = pl.BlockSpec(memory_space=pl.ANY)
    dma = pltpu.SemaphoreType.DMA
    v = pltpu.VMEM
    return pl.pallas_call(
        main_kernel,
        out_shape=(
            jax.ShapeDtypeStruct((length, 128), BF),
            jax.ShapeDtypeStruct((tokens, 128), BF),
        ),
        in_specs=[hbm, vmem, hbm, hbm, hbm, vmem, hbm, hbm, vmem, vmem, vmem, hbm, hbm, hbm],
        out_specs=(vmem,) * 2,
        scratch_shapes=[
            v((length, width), BF),
            v((head, width), BF),
            v((head, width), BF),
            v((head, width), BF),
            v(w_out.shape, BF),
            v((tokens, width), BF),
            v((2, *w_gate.shape[1:]), BF),
            v((2, *w_up.shape[1:]), BF),
            v((2, *w_down.shape[1:]), BF),
            v((length, head), BF),
            v((length, 2 * head), BF),
            v((blocks * 2, width), BF),
            v((blocks, 2, width), BF),
            v((3, tokens, blocks * cap), BF),
            v((length, length), BF),
            v((blocks, 2, width), BF),
            v((GROUPS, 32, 16, width // 2), BF),
            v((GROUPS, 32, 128, 128), BF),
            v((GROUPS, blocks // GROUPS, 32, 128), BF),
            v((blocks, 32, 128), BF),
            v((blocks, length, 2 * head), BF),
            v((16, length // 2, 2 * head), BF),
            v((length, head), F32),
            v((length, 1), F32),
            dma((9,)),
            dma((3,)),
            dma,
            dma((GROUPS,)),
            dma,
            dma((2 * GROUPS, 2, 9)),
            dma((2 * GROUPS,)),
            dma((blocks - 1,)),
            dma,
            dma,
            dma,
            dma,
            dma,
        ],
        compiler_params=pltpu.CompilerParams(
            collective_id=0, has_side_effects=True, vmem_limit_bytes=64000 * 1024
        ),
        name="main",
    )(
        mixer_rows,
        mixer_gain.reshape(1, -1),
        w_query.T,
        w_key.T,
        w_value.T,
        key_shift.reshape(-1, 1, length),
        w_out,
        expert_rows,
        expert_gain.reshape(1, -1),
        routes.T,
        route_weight.T,
        w_gate[0],
        w_up[0],
        w_down[0],
    )


def solution(mesh):
    torus = Mesh(mesh.devices.reshape(16, 2, 4, 4), ("z", "c", "y", "x"))
    return jax.shard_map(
        per_device,
        mesh=torus,
        in_specs=(
            P(EP, None),
            P(),
            P(None, TP),
            P(None, TP),
            P(None, TP),
            P(TP, None),
            P(None, TP),
            P(EP, None),
            P(),
            P(EP, None),
            P(EP, None),
            P(EP, None, TP),
            P(EP, None, TP),
            P(EP, None, TP),
        ),
        out_specs=(P(EP, TP), P(EP, TP)),
        check_vma=False,
    )
```

```python
import jax
import jax.numpy as jnp
from jax import lax
from jax.experimental import pallas as pl
from jax.experimental.pallas import tpu as pltpu
from jax.sharding import Mesh
from jax.sharding import PartitionSpec as P

MESH = pl.DeviceIdType.MESH
EP = ("z", "c")
TP = ("y", "x")
BF = jnp.bfloat16
F32 = jnp.float32

norm_eps = 1e-06
glu_limit = 7.0
glu_alpha = 1.702

OFFSETS = (-1, 0, 1, 2, 8, 7, -7, -6, 6, 5, -5, -4, 4, 3, -3, -2)
GROUPS = 4
OWN = OFFSETS.index(0)


def iota(shape, dim):
    return lax.broadcasted_iota(jnp.int32, shape, dim)


def rms_scale(source, scaling):
    floats = source.astype(F32)
    inverse = lax.rsqrt(jnp.mean(floats * floats, axis=-1, keepdims=True) + norm_eps)
    return (floats * inverse * scaling).astype(BF)


def split_three(value):
    high = value.astype(BF)
    rest = value - high.astype(F32)
    middle = rest.astype(BF)
    low = (rest - middle.astype(F32)).astype(BF)
    return high, middle, low


def columns_of(routes, weights):
    top, tokens = routes.shape
    fill = jnp.zeros((128 - 2 * top, tokens), F32)
    stacked = jnp.concatenate([routes.astype(F32), weights, fill], axis=0)
    return jnp.transpose(stacked)


def places_of(table, top, experts):
    tokens = table.shape[0]
    lanes = iota((tokens, experts), 1).astype(F32)
    hits = jnp.zeros((tokens, experts), F32)
    for k in range(top):
        hits = hits + (table[:, k : k + 1] == lanes).astype(F32)
    earlier = (iota((tokens, tokens), 1) < iota((tokens, tokens), 0)).astype(F32).astype(BF)
    counts = jnp.dot(earlier, hits.astype(BF), preferred_element_type=F32)
    return [
        jnp.sum(jnp.where(table[:, k : k + 1] == lanes, counts, 0.0), axis=1, keepdims=True)
        for k in range(top)
    ]


def selection_of(table, places, top, experts, parity, firsts):
    tokens = table.shape[0]
    slots = iota((tokens, experts * 2), 1).astype(F32)
    select = jnp.zeros((tokens, experts * 2), F32)
    for k in range(top):
        expert = table[:, k : k + 1]
        here = expert - 2.0 * jnp.floor(expert * 0.5) == parity
        for core, first in enumerate(firsts):
            own = places[k] - first
            line = (expert - parity + core) * 2.0 + own
            wanted = jnp.where(here & (own >= 0.0) & (own < 2.0), line, -1.0)
            select = select + (wanted == slots).astype(F32)
    return select.astype(BF)


def combine_of(table, places, top, experts, cap):
    tokens = table.shape[0]
    spots = iota((tokens, experts * cap), 1).astype(F32)
    combine = jnp.zeros((tokens, experts * cap), F32)
    for k in range(top):
        spot = table[:, k : k + 1] * float(cap) + places[k]
        combine = combine + jnp.where(spot == spots, table[:, top + k : top + k + 1], 0.0)
    return split_three(combine)


class Plane:
    def __init__(self, pieces, order, recv, send, here, up):
        self.pieces, self.order = pieces, order
        self.recv, self.send, self.here, self.up = recv, send, here, up
        self.sent = 0

    def piece(self, slot, part):
        return self.pieces.at[self.order(slot, part)]

    def bulk(self, number, recv=None):
        ref = self.pieces.at[pl.ds(0, number)]
        return pltpu.make_async_remote_copy(
            src_ref=ref,
            dst_ref=ref,
            send_sem=self.send,
            recv_sem=self.recv.at[0, 0] if recv is None else recv,
            device_id={"c": 1 - self.here["c"]},
            device_id_type=MESH,
        )

    def slot(self, f, s):
        column = self.here["l"]
        if f:
            column = column + 1 - 2 * lax.rem(column, 2)
        return lax.rem(self.here["y"] + s + 4, 4) * 4 + column

    def put(self, part, f, s, where):
        axis, delta = where
        h = self.here
        if axis == "x":
            target, index = {"x": h["x"] + 1 - 2 * lax.rem(h["x"], 2)}, (1 - f) * 4 + s % 4
        elif axis == "y":
            target, index = {"y": lax.rem(h["y"] + delta + 4, 4)}, f * 4 + (s - delta) % 4
        else:
            target, index = {"c": 1 - h["c"]}, 8
        ref = self.piece(self.slot(f, s), part)
        copy = pltpu.make_async_remote_copy(
            src_ref=ref,
            dst_ref=ref,
            send_sem=self.send,
            recv_sem=self.recv.at[part, index],
            device_id=target,
            device_id_type=MESH,
        )
        copy.start()
        self.sent += 1

    def take(self, part, f, s):
        ref = self.piece(self.slot(f, s), part)
        pltpu.make_async_remote_copy(
            src_ref=ref,
            dst_ref=ref,
            send_sem=self.send,
            recv_sem=self.recv.at[part, f * 4 + s % 4],
            device_id={"c": 1 - self.here["c"]},
            device_id_type=MESH,
        ).wait_recv()

    def along_y(self, part, f):
        for delta in (1, -1):
            self.put(part, f, 0, ("y", delta))

    def stage0a(self):
        self.put(0, 0, 0, ("x", 0))
        self.along_y(1, 0)

    def stage0b(self):
        self.along_y(0, 0)
        self.put(1, 0, 0, ("x", 0))
        for part in range(2):
            self.put(part, 0, 0, ("c", 0))

    def stage1(self):
        up = self.up
        self.take(1, 0, -up)
        self.put(1, 0, -up, ("y", up))
        self.put(1, 0, -up, ("x", 0))
        self.take(0, 1, 0)
        self.along_y(0, 1)
        self.take(1, 0, up)
        self.put(1, 0, up, ("x", 0))
        self.put(0, 1, 0, ("c", 0))
        self.put(1, 0, -up, ("c", 0))
        self.put(1, 0, up, ("c", 0))

    def stage2(self):
        for f, sign in ((0, -self.up), (1, self.up)):
            self.take(0, f, -sign)
            self.put(0, f, -sign, ("y", sign))
            self.put(0, f, -sign, ("c", 0))
            if f == 0:
                self.take(1, 0, 2)
                self.put(1, 0, 2, ("x", 0))
                self.put(1, 0, 2, ("c", 0))

    def stage3(self):
        for f, sign in ((0, -self.up), (1, self.up)):
            self.take(0, f, sign)
            self.put(0, f, sign, ("c", 0))
        for s in (0, -self.up, self.up, 2):
            self.take(1, 1, s)
            self.put(1, 1, s, ("c", 0))

    def stage4(self):
        for f in range(2):
            self.take(0, f, 2)
            self.put(0, f, 2, ("c", 0))

    def stage5(self):
        for part in range(2):
            self.bulk(8, self.recv.at[part, 8]).wait_recv()

    def finish(self):
        self.bulk(self.sent).wait_send()


def main_kernel(
    rows_hbm,
    gain_ref,
    wq_hbm,
    wk_hbm,
    wv_hbm,
    shift_ref,
    out_hbm,
    tokens_hbm,
    token_gain_ref,
    routes_ref,
    weight_ref,
    gate_hbm,
    up_hbm,
    down_hbm,
    mixer_ref,
    expert_ref,
    source_ref,
    wq_ref,
    wk_ref,
    wv_ref,
    out_ref,
    tokens_ref,
    gate_ref,
    up_ref,
    down_ref,
    query_ref,
    packed_ref,
    picked,
    outgoing_ref,
    combine_ref,
    triangle_ref,
    turning_ref,
    arrived,
    rows,
    hidden,
    leaving,
    returned,
    kv,
    heads,
    running,
    carry,
    load_sem,
    trade_recv,
    trade_send,
    sent_recv,
    sent_send,
    plane_recv,
    plane_send,
    kv_recv,
    kv_send,
    head_recv,
    head_send,
    back_recv,
    back_send,
):
    loads = {}
    for n, (name, src, dst) in enumerate(
        (
            ("tokens", tokens_hbm, tokens_ref),
            ("rows", rows_hbm, source_ref),
            ("q", wq_hbm, wq_ref),
            ("k", wk_hbm, wk_ref),
            ("v", wv_hbm, wv_ref),
            ("gate", gate_hbm, gate_ref.at[0]),
            ("up", up_hbm, up_ref.at[0]),
            ("down", down_hbm, down_ref.at[0]),
            ("out", out_hbm, out_ref),
        )
    ):
        loads[name] = pltpu.make_async_copy(src, dst, load_sem.at[n])
        loads[name].start()

    nz = lax.axis_size("z")
    z, c = lax.axis_index("z"), lax.axis_index("c")
    y, x = lax.axis_index("y"), lax.axis_index("x")
    side = x // 2
    traded = lax.rem(side + c, 2)
    column = x + traded * (3 - 2 * x)
    here = {"x": x, "y": y, "c": c, "l": column}
    spot = y * 4 + column
    expert_here = z * 2 + side
    part = y * 4 + x
    device = z * 2 + c
    half_z = nz // 2
    chips = nz // GROUPS

    def at_z(delta):
        return lax.rem(z + delta + nz, nz)

    barrier = pltpu.get_barrier_semaphore()
    peers = 0
    for dz in range(nz):
        for k in range(2):
            if dz or k:
                pl.semaphore_signal(
                    barrier,
                    inc=1,
                    device_id={"z": at_z(dz), "c": lax.rem(c + k, 2)},
                    device_id_type=MESH,
                )
                peers += 1
    for dz in range(nz):
        for k in range(2):
            pl.semaphore_signal(
                barrier,
                inc=1,
                device_id={"z": at_z(dz), "c": lax.rem(c + k, 2), "x": 3 - x},
                device_id_type=MESH,
            )
            peers += 1
    for oy in range(4):
        for ox in range(4):
            if oy or ox:
                pl.semaphore_signal(
                    barrier,
                    inc=1,
                    device_id={"y": lax.rem(y + oy, 4), "x": lax.rem(x + ox, 4)},
                    device_id_type=MESH,
                )
                peers += 1

    top, tokens = routes_ref.shape
    experts = outgoing_ref.shape[0]
    table = columns_of(routes_ref[...], weight_ref[...])
    places = places_of(table, top, experts)
    firsts = [
        (2 * (y * 4 + x + lax.rem(side + core, 2) * (3 - 2 * x))).astype(F32) for core in range(2)
    ]
    select = selection_of(table, places, top, experts, side.astype(F32), firsts)
    loads["tokens"].wait()
    normed_b = rms_scale(tokens_ref[...], token_gain_ref[...])
    picked[...] = lax.dot_general(
        select, normed_b, (((0,), (0,)), ((), ())), preferred_element_type=F32
    ).astype(BF)
    for e in range(experts):
        outgoing_ref[e] = picked[2 * e : 2 * e + 2, :]

    pl.semaphore_wait(barrier, peers)

    def dispatch(o, k):
        zt, ct = at_z(-OFFSETS[o]), lax.rem(c + k, 2)
        return pltpu.make_async_remote_copy(
            src_ref=outgoing_ref.at[zt * 2 + ct],
            dst_ref=arrived.at[o * 2 + c],
            send_sem=sent_send,
            recv_sem=sent_recv.at[o // chips],
            device_id={"z": zt, "c": ct},
            device_id_type=MESH,
        )

    def order_of(group):
        return sorted(range(group * chips, (group + 1) * chips), key=lambda o: -abs(OFFSETS[o]))

    def send_out(group):
        for o in order_of(group):
            for k in range(2):
                if o == OWN and k == 0:
                    continue
                dispatch(o, k).start()
        if group == 0:
            arrived[OWN * 2 + c] = outgoing_ref[device]

    def traded_copy(n):
        src, dst = ((gate_hbm, gate_ref), (up_hbm, up_ref), (down_hbm, down_ref))[n]
        return pltpu.make_async_remote_copy(
            src_ref=src,
            dst_ref=dst.at[1],
            send_sem=trade_send,
            recv_sem=trade_recv.at[n],
            device_id={"x": 3 - x, "c": 1 - c},
            device_id_type=MESH,
        )

    def trade():
        @pl.when(traded == 1)
        def _():
            for n in range(3):
                traded_copy(n).start()

    def traded_in(numbers):
        @pl.when(traded == 1)
        def _():
            for n in numbers:
                traded_copy(n).wait_recv()

    def pass_on(block, src, index, target):
        pltpu.make_async_remote_copy(
            src_ref=src,
            dst_ref=kv.at[block],
            send_sem=kv_send,
            recv_sem=kv_recv.at[index],
            device_id=target,
            device_id_type=MESH,
        ).start()

    def got(block, index):
        pltpu.make_async_remote_copy(
            src_ref=kv.at[block],
            dst_ref=kv.at[block],
            send_sem=kv_send,
            recv_sem=kv_recv.at[index],
            device_id={"c": 1 - c},
            device_id_type=MESH,
        ).wait_recv()

    ups, downs = half_z, half_z - 1
    up0, down0 = -1, ups - 1
    pup0, pdown0 = ups + downs, 2 * ups + downs

    def onward(distance, src, block, sign):
        base, most = (up0, ups) if sign > 0 else (down0, downs)
        for hop in (2, 1):
            if distance + hop <= most:
                pass_on(block, src, base + distance + hop, {"z": at_z(sign * hop)})

    def to_partner(distance, src, block, sign):
        base = pup0 if sign > 0 else pdown0
        pass_on(block, src, base + distance, {"c": 1 - c})

    def arrival(distance, sign):
        block = at_z(-sign * distance) * 2 + c
        got(block, (up0 if sign > 0 else down0) + distance)
        if distance % 2 == 0:
            onward(distance, kv.at[block], block, sign)
        to_partner(distance, kv.at[block], block, sign)

    def ring(step):
        if step == 0:
            onward(0, packed_ref, device, 1)
            onward(0, packed_ref, device, -1)
            to_partner(0, packed_ref, device, 1)
            return
        for distance in (2 * step, 2 * step - 1):
            arrival(distance, 1)
            if distance <= downs:
                arrival(distance, -1)

    def partner(distance, sign=1):
        got(at_z(-sign * distance) * 2 + 1 - c, (pup0 if sign > 0 else pdown0) + distance)

    length, head = query_ref.shape

    def stick(anchor, allowed=None):
        packed = kv[anchor]
        scores = lax.dot_general(
            query_ref[...],
            packed[:, :head],
            (((1,), (1,)), ((), ())),
            preferred_element_type=F32,
        )
        scores = scores + shift_ref[anchor]
        tail = jnp.log(1.0 + jnp.exp(-jnp.abs(scores)))
        soft = jnp.maximum(scores, 0.0) + tail
        if allowed is not None:
            soft = jnp.where(allowed, soft, 0.0)
        after = jnp.dot(soft.astype(BF), triangle_ref[...], preferred_element_type=F32)
        return jnp.minimum(scores, 0.0) - tail - after, after[:, :1] + soft[:, :1], packed[:, head:]

    def values_of(exponent, valued, allowed=None):
        weights = jnp.exp(exponent)
        if allowed is not None:
            weights = jnp.where(allowed, weights, 0.0)
        return jnp.dot(weights.astype(BF), valued, preferred_element_type=F32)

    def attend_diagonal():
        square = (length, length)
        triangle_ref[...] = (iota(square, 0) > iota(square, 1)).astype(F32).astype(BF)
        allowed = iota(square, 1) < iota(square, 0)
        exponent, total, valued = stick(device, allowed)
        running[...] = values_of(exponent, valued, allowed)
        carry[...] = total

    def attend_own():
        @pl.when(c == 1)
        def _():
            exponent, total, valued = stick(device - 1)
            running[...] += values_of(exponent - carry[...], valued)
            carry[...] += total

    def attend(first, last):
        def one(distance, none):
            near = (z - distance) * 2 + 1
            exponent, total, valued = stick(near)
            exponent2, total2, valued2 = stick(near - 1)
            before = carry[...]
            between = before + total
            running[...] += values_of(exponent - before, valued) + values_of(
                exponent2 - between, valued2
            )
            carry[...] = between + total2
            return none

        lax.fori_loop(first, jnp.minimum(last, z) + 1, one, 0)

    def gathering(number, pieces):
        sign = 1 if number % 2 == 0 else -1

        def order(slot, part):
            return part * 16 + slot

        return Plane(pieces, order, plane_recv.at[number], plane_send.at[number], here, sign)

    rows_of = [gathering(n, rows.at[n]) for n in range(GROUPS)]
    hidden_of = [gathering(GROUPS + n, hidden.at[n]) for n in range(GROUPS)]
    gathers = rows_of + hidden_of
    half_width = rows.shape[3]

    def lay_out(group):
        lines = 2 * chips
        ref = arrived.at[pl.ds(0, lines - (group == 0))]
        pltpu.make_async_remote_copy(
            src_ref=ref,
            dst_ref=ref,
            send_sem=sent_send,
            recv_sem=sent_recv.at[group],
            device_id={"c": 1 - c},
            device_id_type=MESH,
        ).wait_recv()
        for line in range(lines):
            for half in range(2):
                rows[group, half * 16 + spot, 2 * line : 2 * line + 2, :] = arrived[
                    group * lines + line, :, half * half_width : (half + 1) * half_width
                ]

    def expand(group):
        both = jnp.concatenate([gate_ref[traded], up_ref[traded]], axis=1)
        units = gate_ref.shape[2]

        def one(n, none):
            first, second = (
                rows[group, pl.ds(half * 16 + n * 8, 8)].reshape(128, half_width)
                for half in range(2)
            )
            flat = jnp.dot(first, both[:half_width], preferred_element_type=F32)
            flat = flat + jnp.dot(second, both[half_width:], preferred_element_type=F32)
            gating = jnp.minimum(flat[:, :units], glu_limit)
            linear = jnp.clip(flat[:, units:], -glu_limit, glu_limit)
            value = gating * jax.nn.sigmoid(glu_alpha * gating) * (linear + 1.0)
            hidden[group, n * 16 + spot] = value.astype(BF)
            return none

        lax.fori_loop(0, 2, one, 0)

    def turning():
        total = turning_ref.shape[0]
        to, of = iota((total, total), 0), iota((total, total), 1)
        source = ((to >> 1) & 15) * 16 + (to >> 5) * 2 + (to & 1)
        turning_ref[...] = (source == of).astype(F32).astype(BF)

    def contract(group):
        total = 256
        result = jnp.zeros((total, 128), F32)
        for pair in range(8):
            units = jnp.concatenate(
                [
                    jnp.concatenate([hidden[group, n], hidden[group, 16 + n]], axis=0)
                    for n in (2 * pair, 2 * pair + 1)
                ],
                axis=1,
            )
            result = result + jnp.dot(
                units,
                down_ref[traded, pair * 256 : (pair + 1) * 256],
                preferred_element_type=F32,
            )
        turned = jnp.dot(
            turning_ref[...], result.astype(BF), preferred_element_type=F32
        ).astype(BF)
        leaving[group] = turned.reshape(2 * chips, 32, 128)

    def send_back(o, k):
        zt, ct = at_z(OFFSETS[o]), lax.rem(c + k, 2)
        group, line = divmod(o, chips)
        return pltpu.make_async_remote_copy(
            src_ref=leaving.at[group, line * 2 + ct],
            dst_ref=returned.at[expert_here],
            send_sem=back_send,
            recv_sem=back_recv,
            device_id={"z": zt, "c": ct, "x": column},
            device_id_type=MESH,
        )

    def give_back(group):
        for o in order_of(group):
            for k in range(2):
                if o == OWN and k == 0:

                    @pl.when(traded == 1)
                    def _():
                        send_back(OWN, 0).start()

                    @pl.when(traded == 0)
                    def _():
                        returned[expert_here] = leaving[0, OWN * 2 + c]

                    continue
                send_back(o, k).start()

    def bulk(ref, send, recv):
        return pltpu.make_async_remote_copy(
            src_ref=ref,
            dst_ref=ref,
            send_sem=send,
            recv_sem=recv,
            device_id={"c": 1 - c},
            device_id_type=MESH,
        )

    def of_all(wait):
        @pl.when(traded == 1)
        def _():
            wait(bulk(returned.at[pl.ds(0, 2 * nz)], back_send, back_recv))

        @pl.when(traded == 0)
        def _():
            wait(bulk(returned.at[pl.ds(0, 2 * nz - 1)], back_send, back_recv))

    def take_back():
        of_all(lambda copy: copy.wait_recv())

    def head_copy(oy, ox):
        return pltpu.make_async_remote_copy(
            src_ref=heads.at[part],
            dst_ref=heads.at[part],
            send_sem=head_send,
            recv_sem=head_recv,
            device_id={"y": lax.rem(y + oy, 4), "x": lax.rem(x + ox, 4)},
            device_id_type=MESH,
        )

    def project():
        for name in ("rows", "q", "k", "v"):
            loads[name].wait()
        normed = rms_scale(source_ref[...], gain_ref[...])

        def product(weight_ref):
            return lax.dot_general(
                normed, weight_ref[...], (((1,), (1,)), ((), ())), preferred_element_type=F32
            ).astype(BF)

        query_ref[...] = product(wq_ref) * BF(head ** (-0.5))
        packed_ref[:, :head] = product(wk_ref)
        packed_ref[:, head:] = product(wv_ref)
        kv[device] = packed_ref[...]

    def tables():
        for n, term in enumerate(combine_of(table, places, top, experts, 32)):
            combine_ref[n] = term

    def send_heads():
        for oy in range(4):
            for ox in range(4):
                if oy or ox:
                    head_copy(oy, ox).start()

    def wait_heads():
        bulk(heads.at[pl.ds(0, 15)], head_send, head_recv).wait_recv()

    def store_heads():
        summed = running[...].astype(BF)
        heads[part, :, :head] = summed[: length // 2]
        heads[part, :, head:] = summed[length // 2 :]

    def mix():
        mixed = jnp.zeros((length, 128), F32)
        for n in range(16):
            pair = heads[n]
            lines = jnp.concatenate([pair[:, :head], pair[:, head:]], axis=0)
            mixed = mixed + jnp.dot(
                lines, out_ref[n * head : (n + 1) * head], preferred_element_type=F32
            )
        mixer_ref[...] = mixed.astype(BF)

    def combine():
        results = returned[...].reshape(-1, 128)
        final = jnp.dot(combine_ref[0], results, preferred_element_type=F32)
        for n in range(1, 3):
            final = final + jnp.dot(combine_ref[n], results, preferred_element_type=F32)
        expert_ref[...] = final.astype(BF)

    def settle():
        bulk(arrived.at[pl.ds(0, 2 * nz - 1)], sent_send, sent_recv.at[0]).wait_send()
        bulk(kv.at[pl.ds(0, 2 * (ups + downs) + 1)], kv_send, kv_recv.at[0]).wait_send()
        bulk(heads.at[pl.ds(0, 15)], head_send, head_recv).wait_send()
        of_all(lambda copy: copy.wait_send())
        for gather in gathers:
            gather.finish()

        @pl.when(traded == 1)
        def _():
            bulk(gate_ref, trade_send, trade_recv.at[0]).wait_send()
            bulk(down_ref.at[0], trade_send, trade_recv.at[0]).wait_send()

    plan = []

    def due(time, name, work, *arguments):
        plan.append((time, len(plan), name, work, arguments))

    def load_weights():
        for name in ("gate", "up", "down", "out"):
            loads[name].wait()

    def expand_and_go(group):
        expand(group)
        hidden_of[group].stage0a()

    def contract_and_go(group):
        contract(group)
        give_back(group)

    def lay_out_and_go(group):
        lay_out(group)
        rows_of[group].stage0a()
        rows_of[group].stage0b()

    def partners(distances, sign=1):
        for distance in distances:
            partner(distance, sign)

    def pass_heads():
        store_heads()
        send_heads()

    def pass_heads_if(finished):
        pl.when(finished)(pass_heads)

    def attend_if(wanted, first, last):
        pl.when(wanted)(lambda: attend(first, last))

    due(0.0, "send", send_out, 0)
    due(0.1, "trade", trade)
    due(0.2, "send", send_out, 1)
    due(0.3, "project", project)
    due(0.4, "send", send_out, 2)
    due(4.0, "send", send_out, 3)
    due(0.6, "diagonal", attend_diagonal)
    due(3.0, "tables", tables)
    due(3.1, "turning", turning)
    due(1.0, "ring", ring, 0)
    due(9.0, "weights", load_weights)
    for group, time in enumerate((5.5, 13.4, 15.0, 19.2)):
        due(time, f"lay{group}", lay_out_and_go, group)
        for kind, gather in (("rows", rows_of[group]), ("hidden", hidden_of[group])):
            tag = f"{kind}{group}"
            due(time + 3.4, tag + "_1", gather.stage1)
            due(time + 6.4, tag + "_2", gather.stage2)
            due(time + 9.2, tag + "_3", gather.stage3)
            due(time + 9.4, tag + "_4", gather.stage4)
            due(time + 11.0, tag + "_5", gather.stage5)
            time = time + 11.8
            if kind == "rows":
                if group == 0:
                    due(time - 0.5, "traded", traded_in, (0, 1))
                due(time - 0.4, f"expand{group}", expand_and_go, group)
                due(time - 0.2, f"hidden{group}_0", hidden_of[group].stage0b)
        if group == 0:
            due(time - 0.5, "traded", traded_in, (2,))
        due(time - 0.4, f"contract{group}", contract_and_go, group)
    due(16.7, "ring", ring, 1)
    due(18.6, "partners", partners, (0, 1, 2))
    due(18.7, "attend", attend_own)
    due(18.8, "attend", attend, 1, 2)
    due(21.6, "ring", ring, 2)
    due(23.8, "partners", partners, (3, 4))
    due(23.9, "attend", attend, 3, 4)
    due(26.6, "ring", ring, 3)
    due(28.75, "partners", partners, (5, 6))
    due(28.76, "attend", attend, 5, 6)
    due(34.45, "ring", ring, 4)
    due(38.3, "partners", partners, (7, 8))
    due(38.31, "attend", attend, 7, 8)
    due(38.32, "partners", partners, tuple(range(1, downs + 1)), -1)
    due(38.33, "attend", attend_if, z <= 10, 9, 10)
    due(42.55, "attend", attend_if, z > 10, 9, 10)
    due(42.6, "attend", attend, 11, 12)
    due(42.61, "attend", attend, 13, nz - 1)
    due(38.34, "heads", pass_heads_if, z <= 10)
    due(42.62, "heads", pass_heads_if, z > 10)
    due(80.0, "wait_heads", wait_heads)
    due(80.1, "mix", mix)
    due(80.2, "take_back", take_back)
    due(80.3, "combine", combine)
    due(80.4, "settle", settle)
    for _, _, name, work, arguments in sorted(plan, key=lambda entry: entry[:2]):
        with jax.named_scope(name):
            work(*arguments)


def per_device(
    mixer_rows,
    mixer_gain,
    w_query,
    w_key,
    w_value,
    key_shift,
    w_out,
    expert_rows,
    expert_gain,
    routes,
    route_weight,
    w_gate,
    w_up,
    w_down,
):
    length, width = mixer_rows.shape
    head = w_query.shape[1]
    tokens = expert_rows.shape[0]
    blocks = lax.axis_size("z") * 2
    cap = 2 * lax.axis_size("y") * lax.axis_size("x")
    vmem = pl.BlockSpec(memory_space=pltpu.VMEM)
    hbm = pl.BlockSpec(memory_space=pl.ANY)
    dma = pltpu.SemaphoreType.DMA
    v = pltpu.VMEM
    return pl.pallas_call(
        main_kernel,
        out_shape=(
            jax.ShapeDtypeStruct((length, 128), BF),
            jax.ShapeDtypeStruct((tokens, 128), BF),
        ),
        in_specs=[hbm, vmem, hbm, hbm, hbm, vmem, hbm, hbm, vmem, vmem, vmem, hbm, hbm, hbm],
        out_specs=(vmem,) * 2,
        scratch_shapes=[
            v((length, width), BF),
            v((head, width), BF),
            v((head, width), BF),
            v((head, width), BF),
            v(w_out.shape, BF),
            v((tokens, width), BF),
            v((2, *w_gate.shape[1:]), BF),
            v((2, *w_up.shape[1:]), BF),
            v((2, *w_down.shape[1:]), BF),
            v((length, head), BF),
            v((length, 2 * head), BF),
            v((blocks * 2, width), BF),
            v((blocks, 2, width), BF),
            v((3, tokens, blocks * cap), BF),
            v((length, length), BF),
            v((256, 256), BF),
            v((blocks, 2, width), BF),
            v((GROUPS, 32, 16, width // 2), BF),
            v((GROUPS, 32, 128, 128), BF),
            v((GROUPS, blocks // GROUPS, 32, 128), BF),
            v((blocks, 32, 128), BF),
            v((blocks, length, 2 * head), BF),
            v((16, length // 2, 2 * head), BF),
            v((length, head), F32),
            v((length, 1), F32),
            dma((9,)),
            dma((3,)),
            dma,
            dma((GROUPS,)),
            dma,
            dma((2 * GROUPS, 2, 9)),
            dma((2 * GROUPS,)),
            dma((blocks - 1,)),
            dma,
            dma,
            dma,
            dma,
            dma,
        ],
        compiler_params=pltpu.CompilerParams(
            collective_id=0, has_side_effects=True, vmem_limit_bytes=64000 * 1024
        ),
        name="main",
    )(
        mixer_rows,
        mixer_gain.reshape(1, -1),
        w_query.T,
        w_key.T,
        w_value.T,
        key_shift.reshape(-1, 1, length),
        w_out,
        expert_rows,
        expert_gain.reshape(1, -1),
        routes.T,
        route_weight.T,
        w_gate[0],
        w_up[0],
        w_down[0],
    )


def solution(mesh):
    torus = Mesh(mesh.devices.reshape(16, 2, 4, 4), ("z", "c", "y", "x"))
    return jax.shard_map(
        per_device,
        mesh=torus,
        in_specs=(
            P(EP, None),
            P(),
            P(None, TP),
            P(None, TP),
            P(None, TP),
            P(TP, None),
            P(None, TP),
            P(EP, None),
            P(),
            P(EP, None),
            P(EP, None),
            P(EP, None, TP),
            P(EP, None, TP),
            P(EP, None, TP),
        ),
        out_specs=(P(EP, TP), P(EP, TP)),
        check_vma=False,
    )
```
